32 devices in a mesh: rep: 2 (over y), fs: 4 (over z), tp: 4 (over x, core).
Axes of the slice: x: 2, y: 2, z: 4, core: 2. Of those that a mesh axis runs over, the one named last changes fastest.
Arguments:
- stream: bfloat16 [2048, 1536], P(('rep', 'fs')), may hold values from -6 to 6
- mix_pre_gain: float32 [1536], replicated, may hold values from 0.1 to 1.9
- w_outer_gate: bfloat16 [1536, 768], P('fs', 'tp'), may hold values from -0.15625 to 0.15625
- w_inner_gate: bfloat16 [1536, 768], P('fs', 'tp'), may hold values from -0.15625 to 0.15625
- w_value: bfloat16 [1536, 768], P('fs', 'tp'), may hold values from -0.15625 to 0.15625
- mix_taps: float32 [3, 768], P(None, 'tp'), may hold values from -3 to 3
- w_mix_out: bfloat16 [768, 1536], P('tp', 'fs'), may hold values from -0.3125 to 0.3125
- mix_post_gain: float32 [1536], replicated, may hold values from 0.1 to 1.9
- ffn_pre_gain: float32 [1536], replicated, may hold values from 0.1 to 1.9
- w_linear: bfloat16 [1536, 4224], P('fs', 'tp'), may hold values from -0.15625 to 0.15625
- w_gated: bfloat16 [1536, 4224], P('fs', 'tp'), may hold values from -0.15625 to 0.15625
- ffn_taps: float32 [3, 4224], P(None, 'tp'), may hold values from -3 to 3
- ffn_bias: float32 [4224], P('tp'), may hold values from -3 to 3
- w_down: bfloat16 [4224, 1536], P('tp', 'fs'), may hold values from -0.125 to 0.125
- ffn_post_gain: float32 [1536], replicated, may hold values from 0.1 to 1.9
Outputs:
- result: bfloat16 [2048, 1536], P(('rep', 'fs'))
The draws below stay inside these ranges and needn't reach their ends.
All inputs are finite; a program needn't handle non-finite values.
Results may differ from the reference program's by a relative error of at most 0.023.
Values may be sent and summed in bfloat16 or wider, within the bound.
A program may use at most 64 MiB of HBM per device.

```python
import jax
import jax.numpy as jnp
from jax import lax

D = 1536
CONV_W = 768
FF = 4224
SEQ_LEN = 128
TOKENS = 2048
N_TP = 4


def spiked(entries, stream_key, source, target, blocks, factor):
    owner, partner = [(jnp.arange(entries.shape[position]) // (entries.shape[position] // blocks)).reshape([-1 if axis == position else 1 for axis in range(entries.ndim)]) for position in (source, target)]
    chosen = jax.random.permutation(stream_key, blocks)[partner]
    strong = (owner == chosen) | (owner == (partner + blocks // 2) % blocks)
    return jnp.where(strong, factor * entries, entries)


def block_levels(own_key, dims, shards, least, largest):
    factor_of, own = 1.0, jax.random.fold_in(own_key, 6)
    for axis_at, shards_of in shards:
        draws = jnp.exp(jax.random.uniform(jax.random.fold_in(own, axis_at), (shards_of,), jnp.float32, least / len(shards), largest / len(shards)))
        factor_of = factor_of * jnp.repeat(draws, dims[axis_at] // shards_of).reshape([-1 if axis == axis_at else 1 for axis in range(len(dims))])
    return factor_of


def scatter_about(stream_key, dims, deviation, limit, cuts=(), held_as=jnp.bfloat16):
    drawn = jax.random.normal(stream_key, dims, jnp.float32) * deviation
    if len(cuts) > 0:
        drawn = block_levels(stream_key, dims, cuts, -0.22, 0.18) * drawn
    return jnp.clip(drawn, min=-limit, max=limit).astype(held_as)


def gaussian_with(own_key, shape, scale, reach, shards, heavy, kind=jnp.bfloat16):
    values = scale * jax.random.normal(own_key, shape, jnp.float32)
    if shards:
        values = values * block_levels(own_key, shape, shards, -0.22, 0.18)
    return jnp.clip(spiked(values, jax.random.fold_in(own_key, 3), *heavy), -reach, reach).astype(kind)


def setup_inputs(seed: int = 0) -> dict:
    streams_of = jax.random.split(jax.random.key(seed), 16)
    stream = scatter_about(streams_of[0], (TOKENS, D), 1.0, 6.0, ((0, 8),))
    mix_pre_gain = jnp.clip(1.0 + 0.18 * jax.random.normal(streams_of[1], (D,), jnp.float32), 0.1, 1.9)
    w_outer_gate = scatter_about(streams_of[2], (D, CONV_W), D ** -0.5, 0.15625, ((0, 4), (1, 4)))
    w_inner_gate = scatter_about(streams_of[3], (D, CONV_W), D ** -0.5, 0.15625, ((0, 4), (1, 4)))
    w_value = scatter_about(streams_of[4], (D, CONV_W), D ** -0.5, 0.15625, ((0, 4), (1, 4)))
    mix_taps = scatter_about(streams_of[5], (3, CONV_W), 0.577, 3.0, ((1, 4),), jnp.float32)
    w_mix_out = gaussian_with(streams_of[6], (CONV_W, D), CONV_W ** -0.5, 0.3125, ((0, 4), (1, 4)), (0, 1, 4, 2.0))
    mix_post_gain = jnp.clip(1.0 + 0.18 * jax.random.normal(streams_of[7], (D,), jnp.float32), 0.1, 1.9)
    ffn_pre_gain = jnp.clip(1.0 + 0.18 * jax.random.normal(streams_of[8], (D,), jnp.float32), 0.1, 1.9)
    w_linear = scatter_about(streams_of[9], (D, FF), D ** -0.5, 0.15625, ((0, 4), (1, 4)))
    w_gated = scatter_about(streams_of[10], (D, FF), D ** -0.5, 0.15625, ((0, 4), (1, 4)))
    ffn_taps = scatter_about(streams_of[11], (3, FF), 0.577, 3.0, ((1, 4),), jnp.float32)
    ffn_bias = scatter_about(streams_of[12], (FF,), 0.5, 3.0, ((0, 4),), jnp.float32)
    w_down = gaussian_with(streams_of[13], (FF, D), FF ** -0.5, 0.125, ((0, 4), (1, 4)), (0, 1, 4, 2.0))
    ffn_post_gain = jnp.clip(1.0 + 0.18 * jax.random.normal(streams_of[14], (D,), jnp.float32), 0.1, 1.9)
    return {"stream": stream, "mix_pre_gain": mix_pre_gain, "w_outer_gate": w_outer_gate, "w_inner_gate": w_inner_gate, "w_value": w_value, "mix_taps": mix_taps, "w_mix_out": w_mix_out, "mix_post_gain": mix_post_gain, "ffn_pre_gain": ffn_pre_gain, "w_linear": w_linear, "w_gated": w_gated, "ffn_taps": ffn_taps, "ffn_bias": ffn_bias, "w_down": w_down, "ffn_post_gain": ffn_post_gain}


EPS = 1e-06

def norm_scale(values, gain):
    return values * lax.rsqrt(lax.optimization_barrier(jnp.mean(values * values, axis=-1, keepdims=True)) + EPS) * gain

def conv_three(values, taps):
    height, breadth = values.shape
    grouped = values.reshape(height // SEQ_LEN, SEQ_LEN, breadth)
    padded = jnp.pad(grouped, ((0, 0), (1, 1), (0, 0)))
    mixed = taps[0] * padded[:, :-2] + taps[1] * padded[:, 1:-1] + taps[2] * padded[:, 2:]
    return mixed.reshape(height, breadth)

def blocked_sum(left, right):
    block_cols = left.shape[1] // N_TP
    summed = jnp.zeros((left.shape[0], right.shape[1]), jnp.float32)
    for block in range(N_TP):
        partial_value = jnp.dot(left[:, block * block_cols:(block + 1) * block_cols], right[block * block_cols:(block + 1) * block_cols], preferred_element_type=jnp.float32)
        rounded = lax.optimization_barrier(partial_value.astype(jnp.bfloat16))
        summed = summed + rounded.astype(jnp.float32)
    return summed.astype(jnp.bfloat16)

def reference(stream, mix_pre_gain, w_outer_gate, w_inner_gate, w_value, mix_taps, w_mix_out, mix_post_gain, ffn_pre_gain, w_linear, w_gated, ffn_taps, ffn_bias, w_down, ffn_post_gain):
    resid = stream.astype(jnp.float32)
    normed = norm_scale(resid, mix_pre_gain).astype(jnp.bfloat16)
    outer = jnp.dot(normed, w_outer_gate, preferred_element_type=jnp.float32).astype(jnp.bfloat16)
    inner = jnp.dot(normed, w_inner_gate, preferred_element_type=jnp.float32).astype(jnp.bfloat16)
    value = jnp.dot(normed, w_value, preferred_element_type=jnp.float32).astype(jnp.bfloat16)
    product = inner.astype(jnp.float32) * value.astype(jnp.float32)
    mixed = (outer.astype(jnp.float32) * conv_three(product, mix_taps)).astype(jnp.bfloat16)
    branch = blocked_sum(mixed, w_mix_out)
    middle = (resid + norm_scale(branch.astype(jnp.float32), mix_post_gain)).astype(jnp.bfloat16)
    middle_f = middle.astype(jnp.float32)
    normed_two = norm_scale(middle_f, ffn_pre_gain).astype(jnp.bfloat16)
    linear = jnp.dot(normed_two, w_linear, preferred_element_type=jnp.float32).astype(jnp.bfloat16)
    gated = jnp.dot(normed_two, w_gated, preferred_element_type=jnp.float32).astype(jnp.bfloat16)
    activated = jax.nn.gelu(conv_three(gated.astype(jnp.float32), ffn_taps) + ffn_bias, approximate=True)
    hidden = (activated * linear.astype(jnp.float32)).astype(jnp.bfloat16)
    branch_two = blocked_sum(hidden, w_down)
    return (middle_f + norm_scale(branch_two.astype(jnp.float32), ffn_post_gain)).astype(jnp.bfloat16)
```

```python
import contextlib
import functools

import jax
import jax.numpy as jnp
from jax import lax
from jax.experimental import pallas as pl
from jax.experimental.pallas import tpu as pltpu
from jax.sharding import PartitionSpec as P

SEQ_LEN = 128
PACK = 16
CHUNKS = 2
SPREAD = 2
TRACE = False


EPS = 1e-06


def norm_scale(values, gain):
    return values * lax.rsqrt(jnp.mean(values * values, axis=-1, keepdims=True) + EPS) * gain


def conv_three(values, taps):
    height, breadth = values.shape
    grouped = values.reshape(height // SEQ_LEN, SEQ_LEN, breadth)
    padded = jnp.pad(grouped, ((0, 0), (1, 1), (0, 0)))
    mixed = taps[0] * padded[:, :-2] + taps[1] * padded[:, 1:-1] + taps[2] * padded[:, 2:]
    return mixed.reshape(height, breadth)


def settle(partial_value, resid, post_gain):
    branch = lax.psum(partial_value.astype(jnp.bfloat16), "tp")
    return (resid + norm_scale(branch.astype(jnp.float32), post_gain)).astype(jnp.bfloat16)


def gather_plan(
    stream,
    mix_pre_gain,
    w_outer_gate,
    w_inner_gate,
    w_value,
    mix_taps,
    w_mix_out,
    mix_post_gain,
    ffn_pre_gain,
    w_linear,
    w_gated,
    ffn_taps,
    ffn_bias,
    w_down,
    ffn_post_gain,
):
    resid = stream.astype(jnp.float32)
    normed = norm_scale(resid, mix_pre_gain).astype(jnp.bfloat16)
    full_outer, full_inner, full_value = (
        lax.all_gather(w_outer_gate, "fs", axis=0, tiled=True),
        lax.all_gather(w_inner_gate, "fs", axis=0, tiled=True),
        lax.all_gather(w_value, "fs", axis=0, tiled=True),
    )
    outer = jnp.dot(normed, full_outer, preferred_element_type=jnp.float32)
    inner = jnp.dot(normed, full_inner, preferred_element_type=jnp.float32)
    value = jnp.dot(normed, full_value, preferred_element_type=jnp.float32)
    outer = outer.astype(jnp.bfloat16)
    inner = inner.astype(jnp.bfloat16)
    value = value.astype(jnp.bfloat16)
    product = inner.astype(jnp.float32) * value.astype(jnp.float32)
    mixed = (outer.astype(jnp.float32) * conv_three(product, mix_taps)).astype(jnp.bfloat16)
    full_mix_out = lax.all_gather(w_mix_out, "fs", axis=1, tiled=True)
    partial_value = jnp.dot(mixed, full_mix_out, preferred_element_type=jnp.float32)
    middle = settle(partial_value, resid, mix_post_gain)
    middle_f = middle.astype(jnp.float32)
    normed_two = norm_scale(middle_f, ffn_pre_gain).astype(jnp.bfloat16)
    full_linear, full_gated = (
        lax.all_gather(w_linear, "fs", axis=0, tiled=True),
        lax.all_gather(w_gated, "fs", axis=0, tiled=True),
    )
    linear = jnp.dot(normed_two, full_linear, preferred_element_type=jnp.float32)
    gated = jnp.dot(normed_two, full_gated, preferred_element_type=jnp.float32)
    linear = linear.astype(jnp.bfloat16)
    gated = gated.astype(jnp.bfloat16)
    activated = jax.nn.gelu(
        conv_three(gated.astype(jnp.float32), ffn_taps) + ffn_bias, approximate=True
    )
    hidden = (activated * linear.astype(jnp.float32)).astype(jnp.bfloat16)
    full_down = lax.all_gather(w_down, "fs", axis=1, tiled=True)
    partial_two = jnp.dot(hidden, full_down, preferred_element_type=jnp.float32)
    return settle(partial_two, middle_f, ffn_post_gain)


def dot_nt(left, right):
    return lax.dot_general(left, right, (((1,), (1,)), ((), ())), preferred_element_type=jnp.float32)


def dot_nn(left, right):
    return jnp.dot(left, right, preferred_element_type=jnp.float32)


def conv_rows(values, taps):
    height = values.shape[0]
    row = lax.broadcasted_iota(jnp.int32, values.shape, 0) % SEQ_LEN
    before = jnp.where(row == 0, 0.0, pltpu.roll(values, 1, 0))
    after = jnp.where(row == SEQ_LEN - 1, 0.0, pltpu.roll(values, height - 1, 0))
    return taps[0:1] * before + taps[1:2] * values + taps[2:3] * after


def norm_rows(values, gain):
    scale = lax.rsqrt(jnp.mean(values * values, axis=-1, keepdims=True) + EPS)
    return values * scale * gain


def scope(name):
    return jax.named_scope(name) if TRACE else contextlib.nullcontext()


def kernel(
    n_fs,
    conv_w,
    low,
    cap,
    stream,
    gain_mix_pre,
    gain_mix_post,
    gain_ffn_pre,
    gain_ffn_post,
    w_outer,
    w_inner,
    w_value,
    w_mix_out,
    mix_taps,
    w_linear,
    w_gated,
    w_down,
    ffn_taps,
    ffn_bias,
    out,
    small_all,
    smalls,
    ffn_w,
    ffn_all,
    mix_all,
    normed,
    pm,
    rm,
    sm,
    rxm,
    middle,
    xs,
    pf,
    rf,
    sf,
    rx,
    tf,
    rz,
    mz_s,
    mz_r,
    my_s,
    my_r,
    mr_s,
    mr_r,
    fz_s,
    fz_r,
    fy_s,
    fy_r,
    fx_s,
    fx_r,
    az_s,
    az_r,
    ap_s,
    ap_r,
    rs_s,
    rs_r,
    rz_s,
    rz_r,
    fin_s,
    fin_r,
):
    r, f, t = lax.axis_index("rep"), lax.axis_index("fs"), lax.axis_index("tp")
    x, c = t // 2, t % 2
    t_core, t_side = 2 * x + 1 - c, 2 * (1 - x) + c
    core, side, other = {"tp": t_core}, {"tp": t_side}, {"rep": 1 - r}
    rows, width = stream.shape[0], w_value.shape[1]
    units = w_linear.shape[1]
    share = rows // 4
    mine = pl.ds(pl.multiple_of(c * share, share), share)
    theirs = pl.ds(pl.multiple_of((1 - c) * share, share), share)
    high = units - low

    near = f < n_fs // 2
    mirror = lambda v: jnp.where(near, v, n_fs - 1 - v)
    inner = jnp.where(near, f, n_fs - 1 - f) == 1
    edge = jnp.logical_not(inner)
    order = [mirror(jnp.where(inner, 0, 1)), mirror(2), mirror(3)]
    goals = [mirror(jnp.where(inner, 2, 1)), mirror(jnp.where(inner, 3, 2)), mirror(jnp.where(inner, 0, 3))]
    upward, downward = mirror(jnp.where(inner, 2, 1)), mirror(0)
    places = [f] + order

    started = []

    def send(src, dst, ss, rs, where):
        return pltpu.make_async_remote_copy(
            src_ref=src,
            dst_ref=dst,
            send_sem=ss,
            recv_sem=rs,
            device_id=where,
            device_id_type=pl.DeviceIdType.MESH,
        )

    def start(copy, when=None):
        started.append((copy, when))
        if when is None:
            copy.start()
        else:
            pl.when(when)(copy.start)

    def wait(copy, name):
        with scope(name):
            copy.wait_recv()

    barrier = pltpu.get_barrier_semaphore()
    peers = [core, side, other] + [{"fs": (f + k) % n_fs} for k in (1, 2, 3)]
    for peer in peers:
        pl.semaphore_signal(barrier, inc=1, device_id=peer, device_id_type=pl.DeviceIdType.MESH)
    for p, piece in enumerate((w_outer, w_inner, w_value, w_mix_out)):
        mix_all[f, p * conv_w : (p + 1) * conv_w] = piece[...]
    with scope("barrier"):
        pl.semaphore_wait(barrier, len(peers))

    mix_half = mix_all.shape[1] // 2
    mix_cut = mix_half // CHUNKS

    def mix_copy(b, h, slot, to):
        at = pl.ds(pl.multiple_of(r * mix_half + h * mix_cut, PACK), mix_cut)
        ref = mix_all.at[b, at]
        return send(ref, ref, mz_s.at[slot], mz_r.at[b, h], {"fs": to})

    for h in range(CHUNKS):
        start(mix_copy(f, h, h, upward))
        start(mix_copy(f, h, CHUNKS + h, downward), inner)

    for p, piece in enumerate((w_linear, w_gated, w_down)):
        for j in range(n_fs):
            ffn_w[j, p, low:cap] = jnp.zeros((cap - low, width), ffn_w.dtype)

        @pl.when(r == 0)
        def _():
            for j in range(n_fs):
                ffn_w[j, p, 0:low] = piece[j, 0:low]

        @pl.when(r == 1)
        def _():
            for j in range(n_fs):
                ffn_w[j, p, 0:high] = piece[j, low:units]

    def ffn_send(i):
        for p in range(3):
            src, dst = ffn_w.at[goals[i], p], ffn_all.at[f, 0, p]
            yield send(src, dst, fz_s.at[i, p], fz_r.at[f, p], {"fs": goals[i]})

    ffn_out = [list(ffn_send(i)) for i in range(3)]
    started += [(copy, None) for copies in ffn_out for copy in copies]

    def ffn_start(*which):
        for i in which:
            for copy in ffn_out[i]:
                copy.start()

    pl.when(edge)(functools.partial(ffn_start, 0, 1, 2))

    def ffn_side(i):
        for p in range(3):
            src = ffn_w.at[f, p] if i == 0 else ffn_all.at[places[i], 0, p]
            dst = ffn_all.at[places[i], 2, p]
            yield send(src, dst, fx_s.at[i, p], fx_r.at[i, p], side)

    fx = [list(ffn_side(i)) for i in range(4)]
    for copy in fx[0]:
        start(copy)
    for p, piece in enumerate((w_linear, w_gated, w_down)):
        ffn_all[f, 0, p] = ffn_w[f, p]
        ffn_all[f, 1, p, low:cap] = jnp.zeros((cap - low, width), ffn_w.dtype)

        @pl.when(r == 0)
        def _():
            ffn_all[f, 1, p, 0:high] = piece[f, low:units]

        @pl.when(r == 1)
        def _():
            ffn_all[f, 1, p, 0:low] = piece[f, 0:low]

    small_all[...] = jnp.zeros(small_all.shape, jnp.float32)
    for j in range(n_fs):
        for half, size in enumerate((low, high)):
            at = j * units + half * low
            small_all[j, half, 0:3, 0:size] = ffn_taps[:, at : at + size]
            small_all[j, half, 3:4, 0:size] = ffn_bias[at : at + size][None]
    smalls[0] = small_all[f, r]
    smalls[1] = small_all[f, 1 - r]
    small_copy = send(smalls.at[0], smalls.at[2], fx_s.at[4, 0], fx_r.at[4, 0], side)
    start(small_copy)

    step_rows = 32

    @pl.loop(0, rows // step_rows)
    def _(i):
        at = pl.ds(pl.multiple_of(i * step_rows, step_rows), step_rows)
        normed[at] = norm_rows(stream[at].astype(jnp.float32), gain_mix_pre[...][None]).astype(jnp.bfloat16)

    flows = [(i, h) for i in range(3) for h in range(CHUNKS)]
    turns = [(i, h) for h in range(CHUNKS) for i in range(2)] + [(2, h) for h in range(CHUNKS)]
    my = []
    for e in range(3 * CHUNKS):
        (i_edge, h_edge), (i_inner, h_inner) = flows[e], turns[e]
        b = jnp.where(inner, order[i_inner], order[i_edge])
        h = jnp.where(inner, h_inner, h_edge)
        onward = downward if i_inner > 0 else upward
        copy = mix_copy(b, h, 2 * CHUNKS + e, onward)
        wait(copy, f"mixz_{e}")
        start(copy, inner)
        at = pl.ds(pl.multiple_of(r * mix_half + h * mix_cut, PACK), mix_cut)
        ref = mix_all.at[b, at]
        my.append(send(ref, ref, my_s.at[e], my_r.at[e], other))
        start(my[e])
        if e == 2 * CHUNKS - 2:
            pl.when(inner)(functools.partial(ffn_start, 0, 1))
    pl.when(inner)(functools.partial(ffn_start, 2))

    fy = []
    for i in range(1, 4):
        fy.append([])
        for p in range(3):
            src, dst = ffn_all.at[places[i], 0, p], ffn_all.at[places[i], 1, p]
            fy[-1].append(send(src, dst, fy_s.at[i - 1, p], fy_r.at[i - 1, p], other))

    def forward(i):
        for p in range(3):
            src = ffn_all.at[places[i], 0, p]
            wait(send(src, src, fz_s.at[i - 1, p], fz_r.at[places[i], p], other), f"ffnz_{i}_{p}")
            fy[i - 1][p].start()
            fx[i][p].start()

    for i in range(1, 4):
        started.extend((copy, None) for copy in fy[i - 1])
        started.extend((copy, None) for copy in fx[i])

    @pl.when(inner)
    def _():
        forward(1)

    for e in range(3 * CHUNKS):
        wait(my[e], f"mixy_{e}")

    mix_core = []
    for k, q in enumerate((1 - x, x)):
        here = pl.ds(pl.multiple_of(q * SEQ_LEN, SEQ_LEN), SEQ_LEN)
        parts = []
        for p in range(3):
            total = 0.0
            for j in range(n_fs):
                total = total + dot_nt(
                    normed[here, j * width : (j + 1) * width], mix_all[j, p * conv_w : (p + 1) * conv_w]
                )
            parts.append(total.astype(jnp.bfloat16).astype(jnp.float32))
        mixed = (parts[0] * conv_rows(parts[1] * parts[2], mix_taps)).astype(jnp.bfloat16)
        for j in range(n_fs):
            pm[k, :, j * width : (j + 1) * width] = dot_nn(
                mixed, mix_all[j, 3 * conv_w : 4 * conv_w]
            ).astype(jnp.bfloat16)
        mix_core.append(send(pm.at[k, theirs], rm.at[k], mr_s.at[k], mr_r.at[k], core))
        start(mix_core[k])

    def mix_sum(k):
        wait(mix_core[k], f"mixcore_{k}")
        return (pm[k, mine].astype(jnp.float32) + rm[k].astype(jnp.float32)).astype(jnp.bfloat16)

    sm[...] = mix_sum(0)
    mix_side = send(sm, rxm, mr_s.at[2], mr_r.at[2], side)
    start(mix_side)

    @pl.when(edge)
    def _():
        forward(1)

    kept = mix_sum(1)
    forward(2)
    wait(mix_side, "mixside")
    branch = (kept.astype(jnp.float32) + rxm[...].astype(jnp.float32)).astype(jnp.bfloat16)
    slot = pl.ds(pl.multiple_of(t * share, share), share)
    mid = stream[slot].astype(jnp.float32) + norm_rows(branch.astype(jnp.float32), gain_mix_post[...][None])
    mid = mid.astype(jnp.bfloat16)
    middle[...] = mid
    xs[f, 0, mine] = norm_rows(mid.astype(jnp.float32), gain_ffn_pre[...][None]).astype(jnp.bfloat16)

    across = [z % 2 == 0 for z in places]
    partner = [{"rep": jnp.where(a, r, 1 - r), "tp": jnp.where(a, t_side, t)} for a in across]
    cut = share // SPREAD

    def piece_of(z, s, a):
        return xs.at[z, s, pl.ds(pl.multiple_of(c * share + a * cut, cut), cut)]

    ag_core, ag_pair, ag_pass = {}, {}, {}

    def spread(i):
        z = places[i]
        for a in range(SPREAD):
            src = piece_of(z, 0, a)
            if i == 0:
                start(send(src, src, az_s.at[0, a], az_r.at[z, a], {"fs": upward}))
                start(send(src, src, az_s.at[1, a], az_r.at[z, a], {"fs": downward}), inner)
            else:
                onward = downward if i > 1 else upward
                copy = send(src, src, az_s.at[1 + i, a], az_r.at[z, a], {"fs": onward})
                wait(copy, f"agz_{i}_{a}")
                start(copy, inner)
            ag_pair[i, a] = send(src, piece_of(z, 1, a), ap_s.at[0, i, a], ap_r.at[0, i, a], partner[i])
            start(ag_pair[i, a])
            ag_core[i, a] = send(src, src, ap_s.at[1, i, a], ap_r.at[1, i, a], core)
            start(ag_core[i, a])

    def pass_on(i):
        for a in range(SPREAD):
            wait(ag_pair[i, a], f"agpair_{i}_{a}")
            src = piece_of(places[i], 1, a)
            ag_pass[i, a] = send(src, src, ap_s.at[2, i, a], ap_r.at[2, i, a], core)
            start(ag_pass[i, a])

    rs_core, rs_pair, rs_z = {}, {}, {}

    def block(i, s):
        for a in range(SPREAD):
            wait((ag_pass if s else ag_core)[i, a], f"agcore_{i}_{s}_{a}")
        z = places[i]
        second = jnp.where(across[i], 1, 2)
        hidden = []
        for h in (0, second):
            linear, gated = 0.0, 0.0
            for j in range(n_fs):
                act = xs[z, s, :, j * width : (j + 1) * width]
                linear = linear + dot_nt(act, ffn_all[j, h, 0])
                gated = gated + dot_nt(act, ffn_all[j, h, 1])
            linear = linear.astype(jnp.bfloat16).astype(jnp.float32)
            gated = gated.astype(jnp.bfloat16).astype(jnp.float32)
            small = smalls[h]
            act = jax.nn.gelu(conv_rows(gated, small) + small[3:4], approximate=True)
            hidden.append((act * linear).astype(jnp.bfloat16))
        for j in range(n_fs):
            total = dot_nn(hidden[0], ffn_all[j, 0, 2]) + dot_nn(hidden[1], ffn_all[j, second, 2])
            pf[i, s, :, j * width : (j + 1) * width] = total.astype(jnp.bfloat16)
        rs_core[i, s] = send(pf.at[i, s, theirs], rf.at[i, s], rs_s.at[0, i, s], rs_r.at[0, i, s], core)
        start(rs_core[i, s])

    def stage_core(i, s):
        wait(rs_core[i, s], f"rscore_{i}_{s}")
        total = pf[i, s, mine].astype(jnp.float32) + rf[i, s].astype(jnp.float32)
        sf[i, s] = total.astype(jnp.bfloat16)
        if s:
            rs_pair[i] = send(sf.at[i, s], rx.at[i], rs_s.at[1, i, 0], rs_r.at[1, i, 0], partner[i])
            start(rs_pair[i])

    def stage_pair(i):
        wait(rs_pair[i], f"rspair_{i}")
        total = (sf[i, 0].astype(jnp.float32) + rx[i].astype(jnp.float32)).astype(jnp.bfloat16)
        tf[i] = total
        if i > 0:
            rs_z[i] = send(tf.at[i], rz.at[f], rz_s.at[i], rz_r.at[f], {"fs": places[i]})
            start(rs_z[i])

    spread(0)
    forward(3)
    spread(1)
    pass_on(0)
    for i in range(1, 4):
        for p in range(3):
            wait(fy[i - 1][p], f"ffny_{i}_{p}")
    for i in range(4):
        for p in range(3):
            wait(fx[i][p], f"ffnx_{i}_{p}")
    wait(small_copy, "small")
    block(0, 0)
    block(0, 1)
    spread(2)
    pass_on(1)
    stage_core(0, 1)
    stage_core(0, 0)
    block(1, 0)
    block(1, 1)
    spread(3)
    pass_on(2)
    stage_core(1, 1)
    stage_core(1, 0)
    stage_pair(0)
    block(2, 0)
    block(2, 1)
    pass_on(3)
    stage_core(2, 1)
    stage_core(2, 0)
    stage_pair(1)
    block(3, 0)
    block(3, 1)
    stage_core(3, 1)
    stage_core(3, 0)
    stage_pair(2)
    stage_pair(3)

    total = tf[0].astype(jnp.float32)
    for i in range(1, 4):
        ref = rz.at[places[i]]
        wait(send(ref, ref, rz_s.at[0], rz_r.at[places[i]], {"fs": places[i]}), f"rz_{i}")
        total = total + rz[places[i]].astype(jnp.float32)
    branch = total.astype(jnp.bfloat16).astype(jnp.float32)
    done = middle[...].astype(jnp.float32) + norm_rows(branch, gain_ffn_post[...][None])
    out[slot] = done.astype(jnp.bfloat16)

    def row_slot(who):
        return out.at[pl.ds(pl.multiple_of(who * share, share), share)]

    own, far = row_slot(t), row_slot(t_side)
    fin_side = send(own, own, fin_s.at[0], fin_r.at[0], side)
    start(fin_side)
    fin_core = send(own, own, fin_s.at[1], fin_r.at[1], core)
    start(fin_core)
    wait(fin_side, "finside")
    fin_pass = send(far, far, fin_s.at[2], fin_r.at[2], core)
    start(fin_pass)
    wait(fin_core, "fincore")
    wait(fin_pass, "finpass")

    with scope("sends"):
        for copy, when in started:
            if when is None:
                copy.wait_send()
            else:
                pl.when(when)(copy.wait_send)


def split_plan(
    n_fs,
    stream,
    mix_pre_gain,
    w_outer_gate,
    w_inner_gate,
    w_value,
    mix_taps,
    w_mix_out,
    mix_post_gain,
    ffn_pre_gain,
    w_linear,
    w_gated,
    ffn_taps,
    ffn_bias,
    w_down,
    ffn_post_gain,
):
    rows, model = stream.shape
    width, conv_w = w_value.shape
    units = w_linear.shape[1] // n_fs
    low = units // 2 // PACK * PACK
    cap = -(-(units - low) // PACK) * PACK
    cut = lambda rows_of: rows_of.reshape(n_fs, units, width)
    share = rows // 4
    half = jnp.bfloat16
    vmem, dma = pltpu.VMEM, pltpu.SemaphoreType.DMA
    return pl.pallas_call(
        functools.partial(kernel, n_fs, conv_w, low, cap),
        out_shape=jax.ShapeDtypeStruct((rows, model), half),
        in_specs=[pl.BlockSpec(memory_space=vmem)] * 15,
        out_specs=pl.BlockSpec(memory_space=vmem),
        scratch_shapes=[
            vmem((n_fs, 2, 8, cap), jnp.float32),
            vmem((3, 8, cap), jnp.float32),
            vmem((n_fs, 3, cap, width), half),
            vmem((n_fs, 3, 3, cap, width), half),
            vmem((n_fs, 4 * conv_w, width), half),
            vmem((rows, model), half),
            vmem((2, SEQ_LEN, model), half),
            vmem((2, share, model), half),
            vmem((share, model), half),
            vmem((share, model), half),
            vmem((share, model), half),
            vmem((n_fs, 2, SEQ_LEN, model), half),
            vmem((n_fs, 2, SEQ_LEN, model), half),
            vmem((n_fs, 2, share, model), half),
            vmem((n_fs, 2, share, model), half),
            vmem((n_fs, share, model), half),
            vmem((n_fs, share, model), half),
            vmem((n_fs, share, model), half),
            dma((5 * CHUNKS,)),
            dma((n_fs, CHUNKS)),
            dma((3 * CHUNKS,)),
            dma((3 * CHUNKS,)),
            dma((3,)),
            dma((3,)),
            dma((3, 3)),
            dma((n_fs, 3)),
            dma((3, 3)),
            dma((3, 3)),
            dma((5, 3)),
            dma((5, 3)),
            dma((5, SPREAD)),
            dma((n_fs, SPREAD)),
            dma((3, n_fs, SPREAD)),
            dma((3, n_fs, SPREAD)),
            dma((2, n_fs, 2)),
            dma((2, n_fs, 2)),
            dma((n_fs,)),
            dma((n_fs,)),
            dma((3,)),
            dma((3,)),
        ],
        compiler_params=pltpu.CompilerParams(
            collective_id=0, has_side_effects=True, vmem_limit_bytes=56 * 2**20
        ),
    )(
        stream,
        mix_pre_gain,
        mix_post_gain,
        ffn_pre_gain,
        ffn_post_gain,
        w_outer_gate.T,
        w_inner_gate.T,
        w_value.T,
        w_mix_out,
        mix_taps,
        cut(w_linear.T),
        cut(w_gated.T),
        cut(w_down),
        ffn_taps,
        ffn_bias,
    )


def on_device(rep, n_fs, n_tp, *arrays):
    stream, w_value, w_linear = arrays[0], arrays[4], arrays[9]
    same = n_fs == n_tp == 2 * rep == 4
    whole = w_value.shape[0] % 128 == 0 and w_value.shape[1] % (CHUNKS * PACK) == 0
    even = w_linear.shape[1] % (8 * n_fs) == 0 and stream.shape[0] == 2 * SEQ_LEN
    if same and whole and even:
        return split_plan(n_fs, *arrays)
    return gather_plan(*arrays)


def solution(mesh):
    in_specs = (
        P(("rep", "fs"), None),
        P(),
        P("fs", "tp"),
        P("fs", "tp"),
        P("fs", "tp"),
        P(None, "tp"),
        P("tp", "fs"),
        P(),
        P(),
        P("fs", "tp"),
        P("fs", "tp"),
        P(None, "tp"),
        P("tp"),
        P("tp", "fs"),
        P(),
    )
    out_specs = P(("rep", "fs"), None)
    sizes = mesh.shape
    body = functools.partial(on_device, sizes["rep"], sizes["fs"], sizes["tp"])
    return jax.shard_map(
        body, mesh=mesh, in_specs=in_specs, out_specs=out_specs, check_vma=False
    )
```

```python
import contextlib
import functools

import jax
import jax.numpy as jnp
from jax import lax
from jax.experimental import pallas as pl
from jax.experimental.pallas import tpu as pltpu
from jax.sharding import PartitionSpec as P

SEQ_LEN = 128
PACK = 16
CHUNKS = 4
SPREAD = 2
PARTS = 2
EDGE = (
    (),
    ((3, 0), (3, 1), (3, 2), (1, 0)),
    ((1, 1), (1, 2), (2, 0), (2, 1), (2, 2)),
)
INNER = (
    ((1, 0), (1, 1), (1, 2)),
    ((3, 0), (3, 1), (3, 2)),
    ((2, 0), (2, 1), (2, 2)),
)
SIDEWAYS = (False, True, False, True)
TRACE = False


EPS = 1e-06


def norm_scale(values, gain):
    return values * lax.rsqrt(jnp.mean(values * values, axis=-1, keepdims=True) + EPS) * gain


def conv_three(values, taps):
    height, breadth = values.shape
    grouped = values.reshape(height // SEQ_LEN, SEQ_LEN, breadth)
    padded = jnp.pad(grouped, ((0, 0), (1, 1), (0, 0)))
    mixed = taps[0] * padded[:, :-2] + taps[1] * padded[:, 1:-1] + taps[2] * padded[:, 2:]
    return mixed.reshape(height, breadth)


def settle(partial_value, resid, post_gain):
    branch = lax.psum(partial_value.astype(jnp.bfloat16), "tp")
    return (resid + norm_scale(branch.astype(jnp.float32), post_gain)).astype(jnp.bfloat16)


def gather_plan(
    stream,
    mix_pre_gain,
    w_outer_gate,
    w_inner_gate,
    w_value,
    mix_taps,
    w_mix_out,
    mix_post_gain,
    ffn_pre_gain,
    w_linear,
    w_gated,
    ffn_taps,
    ffn_bias,
    w_down,
    ffn_post_gain,
):
    resid = stream.astype(jnp.float32)
    normed = norm_scale(resid, mix_pre_gain).astype(jnp.bfloat16)
    full_outer, full_inner, full_value = (
        lax.all_gather(w_outer_gate, "fs", axis=0, tiled=True),
        lax.all_gather(w_inner_gate, "fs", axis=0, tiled=True),
        lax.all_gather(w_value, "fs", axis=0, tiled=True),
    )
    outer = jnp.dot(normed, full_outer, preferred_element_type=jnp.float32)
    inner = jnp.dot(normed, full_inner, preferred_element_type=jnp.float32)
    value = jnp.dot(normed, full_value, preferred_element_type=jnp.float32)
    outer = outer.astype(jnp.bfloat16)
    inner = inner.astype(jnp.bfloat16)
    value = value.astype(jnp.bfloat16)
    product = inner.astype(jnp.float32) * value.astype(jnp.float32)
    mixed = (outer.astype(jnp.float32) * conv_three(product, mix_taps)).astype(jnp.bfloat16)
    full_mix_out = lax.all_gather(w_mix_out, "fs", axis=1, tiled=True)
    partial_value = jnp.dot(mixed, full_mix_out, preferred_element_type=jnp.float32)
    middle = settle(partial_value, resid, mix_post_gain)
    middle_f = middle.astype(jnp.float32)
    normed_two = norm_scale(middle_f, ffn_pre_gain).astype(jnp.bfloat16)
    full_linear, full_gated = (
        lax.all_gather(w_linear, "fs", axis=0, tiled=True),
        lax.all_gather(w_gated, "fs", axis=0, tiled=True),
    )
    linear = jnp.dot(normed_two, full_linear, preferred_element_type=jnp.float32)
    gated = jnp.dot(normed_two, full_gated, preferred_element_type=jnp.float32)
    linear = linear.astype(jnp.bfloat16)
    gated = gated.astype(jnp.bfloat16)
    activated = jax.nn.gelu(
        conv_three(gated.astype(jnp.float32), ffn_taps) + ffn_bias, approximate=True
    )
    hidden = (activated * linear.astype(jnp.float32)).astype(jnp.bfloat16)
    full_down = lax.all_gather(w_down, "fs", axis=1, tiled=True)
    partial_two = jnp.dot(hidden, full_down, preferred_element_type=jnp.float32)
    return settle(partial_two, middle_f, ffn_post_gain)


def dot_nt(left, right):
    return lax.dot_general(left, right, (((1,), (1,)), ((), ())), preferred_element_type=jnp.float32)


def dot_nn(left, right):
    return jnp.dot(left, right, preferred_element_type=jnp.float32)


def conv_rows(values, taps):
    height = values.shape[0]
    row = lax.broadcasted_iota(jnp.int32, values.shape, 0) % SEQ_LEN
    before = jnp.where(row == 0, 0.0, pltpu.roll(values, 1, 0))
    after = jnp.where(row == SEQ_LEN - 1, 0.0, pltpu.roll(values, height - 1, 0))
    return taps[0:1] * before + taps[1:2] * values + taps[2:3] * after


def norm_rows(values, gain):
    scale = lax.rsqrt(jnp.mean(values * values, axis=-1, keepdims=True) + EPS)
    return values * scale * gain


def scope(name):
    return jax.named_scope(name) if TRACE else contextlib.nullcontext()


def kernel(n_fs, conv_w, low, cap, *refs):
    sources, out, scratch = refs[:15], refs[15], refs[16:]
    (
        stream,
        gain_mix_pre,
        gain_mix_post,
        gain_ffn_pre,
        gain_ffn_post,
        mix_taps,
        w_linear,
        w_gated,
        w_down,
        ffn_taps,
        ffn_bias,
        load_s,
        small_all,
        smalls,
        ffn_w,
        ffn_all,
        mix_all,
        normed,
        acc,
        pm,
        rm,
        sm,
        rxm,
        middle,
        xs,
        pf,
        rf,
        sf,
        rx,
        tf,
        rz,
        mz_s,
        mz_r,
        my_s,
        my_r,
        mr_s,
        mr_r,
        fz_s,
        fz_r,
        fy_s,
        fy_r,
        fx_s,
        fx_r,
        az_s,
        az_r,
        ap_s,
        ap_r,
        rs_s,
        rs_r,
        rp_s,
        rp_r,
        rz_s,
        rz_r,
        fin_s,
        fin_r,
    ) = scratch
    r, f, t = lax.axis_index("rep"), lax.axis_index("fs"), lax.axis_index("tp")
    x, c = t // 2, t % 2
    t_core, t_side = 2 * x + 1 - c, 2 * (1 - x) + c
    core, side, other = {"tp": t_core}, {"tp": t_side}, {"rep": 1 - r}
    rows, width = stream.shape[0], ffn_w.shape[3]
    units = w_linear.shape[1]
    share = rows // 4
    mine = pl.ds(pl.multiple_of(c * share, share), share)
    theirs = pl.ds(pl.multiple_of((1 - c) * share, share), share)
    high = units - low

    near = f < n_fs // 2
    mirror = lambda v: jnp.where(near, v, n_fs - 1 - v)
    inner = jnp.where(near, f, n_fs - 1 - f) == 1
    edge = jnp.logical_not(inner)
    order = [mirror(jnp.where(inner, 0, 1)), mirror(2), mirror(3)]
    goals = [mirror(jnp.where(inner, 2, 1)), mirror(jnp.where(inner, 3, 2)), mirror(jnp.where(inner, 0, 3))]
    upward, downward = mirror(jnp.where(inner, 2, 1)), mirror(0)
    places = [f] + order

    started = []

    def send(src, dst, ss, rs, where):
        return pltpu.make_async_remote_copy(
            src_ref=src,
            dst_ref=dst,
            send_sem=ss,
            recv_sem=rs,
            device_id=where,
            device_id_type=pl.DeviceIdType.MESH,
        )

    def start(copy, when=None):
        started.append((copy, when))
        if when is None:
            copy.start()
        else:
            pl.when(when)(copy.start)

    def flush(count=None):
        with scope("sends"):
            for copy, when in started[:count]:
                if when is None:
                    copy.wait_send()
                else:
                    pl.when(when)(copy.wait_send)
        del started[:count]

    def wait(copy, name):
        with scope(name):
            copy.wait_recv()

    barrier = pltpu.get_barrier_semaphore()
    peers = [core, side, other] + [{"fs": (f + k) % n_fs} for k in (1, 2, 3)]
    for peer in peers:
        pl.semaphore_signal(barrier, inc=1, device_id=peer, device_id_type=pl.DeviceIdType.MESH)
    targets = [mix_all.at[f, p * conv_w : (p + 1) * conv_w] for p in range(4)]
    targets += [stream, gain_mix_pre, w_linear, w_gated, w_down, ffn_taps, ffn_bias]
    targets += [gain_mix_post, gain_ffn_pre, gain_ffn_post, mix_taps]
    places_in = (5, 6, 7, 8, 0, 1, 10, 11, 12, 13, 14, 2, 3, 4, 9)
    loads = [pltpu.make_async_copy(sources[i], ref, load_s.at[i]) for i, ref in zip(places_in, targets)]
    for load in loads:
        load.start()
    for load in loads[:4]:
        load.wait()
    with scope("barrier"):
        pl.semaphore_wait(barrier, len(peers))

    mix_half = mix_all.shape[1] // 2
    mix_cut = mix_half // CHUNKS

    def mix_copy(b, h, slot, to):
        at = pl.ds(pl.multiple_of(r * mix_half + h * mix_cut, PACK), mix_cut)
        ref = mix_all.at[b, at]
        return send(ref, ref, mz_s.at[slot], mz_r.at[b, h], {"fs": to})

    for h in range(CHUNKS):
        start(mix_copy(f, h, h, upward))
        start(mix_copy(f, h, CHUNKS + h, downward), inner)

    for load in loads[6:]:
        load.wait()

    for p, piece in enumerate((w_linear, w_gated, w_down)):
        for j in range(n_fs):
            ffn_w[j, p, low:cap] = jnp.zeros((cap - low, width), ffn_w.dtype)

        @pl.when(r == 0)
        def _():
            for j in range(n_fs):
                ffn_w[j, p, 0:low] = piece[j, 0:low]

        @pl.when(r == 1)
        def _():
            for j in range(n_fs):
                ffn_w[j, p, 0:high] = piece[j, low:units]

    def ffn_send(i):
        for p in range(3):
            src, dst = ffn_w.at[goals[i], p], ffn_all.at[f, 0, p]
            yield send(src, dst, fz_s.at[i, p], fz_r.at[f, p], {"fs": goals[i]})

    ffn_out = [list(ffn_send(i)) for i in range(3)]
    started += [(copy, None) for copies in ffn_out for copy in copies]

    def ffn_start(*which):
        for i in which:
            for copy in ffn_out[i]:
                copy.start()

    pl.when(edge)(functools.partial(ffn_start, 0, 1, 2))

    def ffn_side(i):
        for p in range(3):
            src = ffn_w.at[f, p] if i == 0 else ffn_all.at[places[i], 0, p]
            dst = ffn_all.at[places[i], 2, p]
            yield send(src, dst, fx_s.at[i, p], fx_r.at[i, p], side)

    fx = [list(ffn_side(i)) for i in range(4)]
    for copy in fx[0]:
        start(copy)
    for p, piece in enumerate((w_linear, w_gated, w_down)):
        ffn_all[f, 0, p] = ffn_w[f, p]
        ffn_all[f, 1, p, low:cap] = jnp.zeros((cap - low, width), ffn_w.dtype)

        @pl.when(r == 0)
        def _():
            ffn_all[f, 1, p, 0:high] = piece[f, low:units]

        @pl.when(r == 1)
        def _():
            ffn_all[f, 1, p, 0:low] = piece[f, 0:low]

    small_all[...] = jnp.zeros(small_all.shape, jnp.float32)
    for j in range(n_fs):
        for half, size in enumerate((low, high)):
            at = j * units + half * low
            small_all[j, half, 0:3, 0:size] = ffn_taps[:, at : at + size]
            small_all[j, half, 3:4, 0:size] = ffn_bias[at : at + size][None]
    smalls[0] = small_all[f, r]
    smalls[1] = small_all[f, 1 - r]
    small_copy = send(smalls.at[0], smalls.at[2], fx_s.at[4, 0], fx_r.at[4, 0], side)
    start(small_copy)

    for load in loads[4:6]:
        load.wait()
    step_rows = 32

    @pl.loop(0, rows // step_rows)
    def _(i):
        at = pl.ds(pl.multiple_of(i * step_rows, step_rows), step_rows)
        value = norm_rows(stream[at].astype(jnp.float32), gain_mix_pre[...][None]).astype(jnp.bfloat16)
        for j in range(n_fs):
            normed[j, at] = value[:, j * width : (j + 1) * width]

    def project(z, first=False):
        for p in range(3):
            term = dot_nt(normed[z], mix_all[z, p * conv_w : (p + 1) * conv_w])
            acc[p] = term if first else acc[p] + term

    project(f, True)

    flows = [(i, h) for i in range(3) for h in range(CHUNKS)]
    turns = [(i, h) for h in range(CHUNKS) for i in range(2)] + [(2, h) for h in range(CHUNKS)]
    my = []
    for e in range(3 * CHUNKS):
        (i_edge, h_edge), (i_inner, h_inner) = flows[e], turns[e]
        b = jnp.where(inner, order[i_inner], order[i_edge])
        h = jnp.where(inner, h_inner, h_edge)
        onward = downward if i_inner > 0 else upward
        copy = mix_copy(b, h, 2 * CHUNKS + e, onward)
        wait(copy, f"mixz_{e}")
        start(copy, inner)
        at = pl.ds(pl.multiple_of(r * mix_half + h * mix_cut, PACK), mix_cut)
        ref = mix_all.at[b, at]
        my.append(send(ref, ref, my_s.at[e], my_r.at[e], other))
        start(my[e])
        if e == 2 * CHUNKS - 2:
            pl.when(inner)(functools.partial(ffn_start, 0, 1))
    pl.when(inner)(functools.partial(ffn_start, 2))

    fy = []
    for i in range(1, 4):
        fy.append([])
        for p in range(3):
            src, dst = ffn_all.at[places[i], 0, p], ffn_all.at[places[i], 1, p]
            fy[-1].append(send(src, dst, fy_s.at[i - 1, p], fy_r.at[i - 1, p], other))

    def forward(*which):
        for i, p in which:
            src = ffn_all.at[places[i], 0, p]
            wait(send(src, src, fz_s.at[i - 1, p], fz_r.at[places[i], p], other), f"ffnz_{i}_{p}")
            fy[i - 1][p].start()
            fx[i][p].start()

    def relay(edge_list, inner_list):
        pl.when(edge)(functools.partial(forward, *edge_list))
        pl.when(inner)(functools.partial(forward, *inner_list))

    for i in range(1, 4):
        started.extend((copy, None) for copy in fy[i - 1])
        started.extend((copy, None) for copy in fx[i])

    relay(EDGE[0], INNER[0])
    for e in range(3 * CHUNKS):
        wait(my[e], f"mixy_{e}")
        if e == 2 * CHUNKS - 1:
            project(order[0])
            project(order[1])
    project(order[2])

    mix_core = []
    for k, q in enumerate((1 - x, x)):
        here = pl.ds(pl.multiple_of(q * SEQ_LEN, SEQ_LEN), SEQ_LEN)
        parts = [acc[p, here].astype(jnp.bfloat16).astype(jnp.float32) for p in range(3)]
        mixed = (parts[0] * conv_rows(parts[1] * parts[2], mix_taps)).astype(jnp.bfloat16)
        for j in range(n_fs):
            pm[k, :, j * width : (j + 1) * width] = dot_nn(
                mixed, mix_all[j, 3 * conv_w : 4 * conv_w]
            ).astype(jnp.bfloat16)
        mix_core.append(send(pm.at[k, theirs], rm.at[k], mr_s.at[k], mr_r.at[k], core))
        start(mix_core[k])

    def mix_sum(k):
        wait(mix_core[k], f"mixcore_{k}")
        return (pm[k, mine].astype(jnp.float32) + rm[k].astype(jnp.float32)).astype(jnp.bfloat16)

    sm[...] = mix_sum(0)
    mix_side = send(sm, rxm, mr_s.at[2], mr_r.at[2], side)
    start(mix_side)

    kept = mix_sum(1)
    relay(EDGE[1], INNER[1])
    wait(mix_side, "mixside")
    branch = (kept.astype(jnp.float32) + rxm[...].astype(jnp.float32)).astype(jnp.bfloat16)
    slot = pl.ds(pl.multiple_of(t * share, share), share)
    mid = stream[slot].astype(jnp.float32) + norm_rows(branch.astype(jnp.float32), gain_mix_post[...][None])
    mid = mid.astype(jnp.bfloat16)
    middle[...] = mid
    xs[f, 0, mine] = norm_rows(mid.astype(jnp.float32), gain_ffn_pre[...][None]).astype(jnp.bfloat16)

    partner = [side if SIDEWAYS[i] else other for i in range(4)]
    cut = share // SPREAD

    def piece_of(z, s, a):
        return xs.at[z, s, pl.ds(pl.multiple_of(c * share + a * cut, cut), cut)]

    ag_core, ag_pair, ag_pass = {}, {}, {}

    def spread(i):
        z = places[i]
        for a in range(SPREAD):
            src = piece_of(z, 0, a)
            if i == 0:
                start(send(src, src, az_s.at[0, a], az_r.at[z, a], {"fs": upward}))
                start(send(src, src, az_s.at[1, a], az_r.at[z, a], {"fs": downward}), inner)
            else:
                onward = downward if i > 1 else upward
                copy = send(src, src, az_s.at[1 + i, a], az_r.at[z, a], {"fs": onward})
                wait(copy, f"agz_{i}_{a}")
                start(copy, inner)
            ag_pair[i, a] = send(src, piece_of(z, 1, a), ap_s.at[0, i, a], ap_r.at[0, i, a], partner[i])
            start(ag_pair[i, a])
            ag_core[i, a] = send(src, src, ap_s.at[1, i, a], ap_r.at[1, i, a], core)
            start(ag_core[i, a])

    def pass_on(i):
        for a in range(SPREAD):
            wait(ag_pair[i, a], f"agpair_{i}_{a}")
            src = piece_of(places[i], 1, a)
            ag_pass[i, a] = send(src, src, ap_s.at[2, i, a], ap_r.at[2, i, a], core)
            start(ag_pass[i, a])

    rs_core, rs_pair, rs_z = {}, {}, {}
    part = share // PARTS

    def block(i, s):
        for a in range(SPREAD):
            wait((ag_pass if s else ag_core)[i, a], f"agcore_{i}_{s}_{a}")
        z = places[i]
        second = 1 if SIDEWAYS[i] else 2
        hidden = []
        for h in (0, second):
            linear, gated = 0.0, 0.0
            for j in range(n_fs):
                act = xs[z, s, :, j * width : (j + 1) * width]
                linear = linear + dot_nt(act, ffn_all[j, h, 0])
                gated = gated + dot_nt(act, ffn_all[j, h, 1])
            linear = linear.astype(jnp.bfloat16).astype(jnp.float32)
            gated = gated.astype(jnp.bfloat16).astype(jnp.float32)
            small = smalls[h]
            act = jax.nn.gelu(conv_rows(gated, small) + small[3:4], approximate=True)
            hidden.append((act * linear).astype(jnp.bfloat16))
        for j in range(n_fs):
            total = dot_nn(hidden[0], ffn_all[j, 0, 2]) + dot_nn(hidden[1], ffn_all[j, second, 2])
            pf[i, s, :, j * width : (j + 1) * width] = total.astype(jnp.bfloat16)
        rs_core[i, s] = send(pf.at[i, s, theirs], rf.at[i, s], rs_s.at[0, i, s], rs_r.at[0, i, s], core)
        start(rs_core[i, s])

    def stage_core(i, s):
        wait(rs_core[i, s], f"rscore_{i}_{s}")
        for a in range(PARTS):
            at = pl.ds(a * part, part)
            ours = pl.ds(pl.multiple_of(c * share + a * part, part), part)
            total = pf[i, s, ours].astype(jnp.float32) + rf[i, s, at].astype(jnp.float32)
            sf[i, s, at] = total.astype(jnp.bfloat16)
            if s:
                rs_pair[i, a] = send(sf.at[i, s, at], rx.at[i, at], rp_s.at[i, a], rp_r.at[i, a], partner[i])
                start(rs_pair[i, a])

    def stage_pair(i):
        for a in range(PARTS):
            at = pl.ds(a * part, part)
            wait(rs_pair[i, a], f"rspair_{i}_{a}")
            tf[i, at] = (sf[i, 0, at].astype(jnp.float32) + rx[i, at].astype(jnp.float32)).astype(jnp.bfloat16)
            if i > 0:
                copy = send(tf.at[i, at], rz.at[f, at], rz_s.at[i, a], rz_r.at[f, a], {"fs": places[i]})
                start(copy)

    spread(0)
    relay(EDGE[2], INNER[2])
    pass_on(0)
    spread(1)
    spread(2)
    for i in range(1, 4):
        for p in range(3):
            wait(fy[i - 1][p], f"ffny_{i}_{p}")
    for i in range(4):
        for p in range(3):
            wait(fx[i][p], f"ffnx_{i}_{p}")
    wait(small_copy, "small")
    block(0, 0)
    pass_on(1)
    block(0, 1)
    block(1, 0)
    stage_core(0, 1)
    stage_core(0, 0)
    spread(3)
    block(1, 1)
    pass_on(2)
    block(2, 0)
    early = len(started)
    stage_core(1, 1)
    stage_core(1, 0)
    block(2, 1)
    stage_pair(0)
    block(3, 0)
    pass_on(3)
    stage_core(2, 1)
    stage_core(2, 0)
    block(3, 1)
    stage_pair(1)
    stage_core(3, 1)
    stage_core(3, 0)
    stage_pair(2)
    flush(early)
    stage_pair(3)

    def row_slot(who, a):
        return pl.ds(pl.multiple_of(who * share + a * part, part), part)

    fin = {}
    for a in range(PARTS):
        at = pl.ds(a * part, part)
        total = tf[0, at].astype(jnp.float32)
        for i in range(1, 4):
            ref = rz.at[places[i], at]
            wait(send(ref, ref, rz_s.at[0, a], rz_r.at[places[i], a], {"fs": places[i]}), f"rz_{i}_{a}")
            total = total + rz[places[i], at].astype(jnp.float32)
        branch = total.astype(jnp.bfloat16).astype(jnp.float32)
        done = middle[at].astype(jnp.float32) + norm_rows(branch, gain_ffn_post[...][None])
        out[row_slot(t, a)] = done.astype(jnp.bfloat16)
        own = out.at[row_slot(t, a)]
        for k, to in enumerate((side, core)):
            fin[k, a] = send(own, own, fin_s.at[k, a], fin_r.at[k, a], to)
            start(fin[k, a])
    for a in range(PARTS):
        wait(fin[0, a], f"finside_{a}")
        far = out.at[row_slot(t_side, a)]
        fin[2, a] = send(far, far, fin_s.at[2, a], fin_r.at[2, a], core)
        start(fin[2, a])
    for a in range(PARTS):
        wait(fin[1, a], f"fincore_{a}")
        wait(fin[2, a], f"finpass_{a}")

    flush()


def split_plan(
    n_fs,
    stream,
    mix_pre_gain,
    w_outer_gate,
    w_inner_gate,
    w_value,
    mix_taps,
    w_mix_out,
    mix_post_gain,
    ffn_pre_gain,
    w_linear,
    w_gated,
    ffn_taps,
    ffn_bias,
    w_down,
    ffn_post_gain,
):
    rows, model = stream.shape
    width, conv_w = w_value.shape
    units = w_linear.shape[1] // n_fs
    low = units // 2 // PACK * PACK
    cap = -(-(units - low) // PACK) * PACK
    cut = lambda rows_of: rows_of.reshape(n_fs, units, width)
    share = rows // 4
    half = jnp.bfloat16
    vmem, dma = pltpu.VMEM, pltpu.SemaphoreType.DMA
    return pl.pallas_call(
        functools.partial(kernel, n_fs, conv_w, low, cap),
        out_shape=jax.ShapeDtypeStruct((rows, model), half),
        in_specs=[pl.BlockSpec(memory_space=pl.ANY)] * 15,
        out_specs=pl.BlockSpec(memory_space=vmem),
        scratch_shapes=[
            vmem((rows, model), half),
            vmem((model,), jnp.float32),
            vmem((model,), jnp.float32),
            vmem((model,), jnp.float32),
            vmem((model,), jnp.float32),
            vmem(mix_taps.shape, jnp.float32),
            vmem((n_fs, units, width), half),
            vmem((n_fs, units, width), half),
            vmem((n_fs, units, width), half),
            vmem(ffn_taps.shape, jnp.float32),
            vmem(ffn_bias.shape, jnp.float32),
            dma((15,)),
            vmem((n_fs, 2, 8, cap), jnp.float32),
            vmem((3, 8, cap), jnp.float32),
            vmem((n_fs, 3, cap, width), half),
            vmem((n_fs, 3, 3, cap, width), half),
            vmem((n_fs, 4 * conv_w, width), half),
            vmem((n_fs, rows, width), half),
            vmem((3, rows, conv_w), jnp.float32),
            vmem((2, SEQ_LEN, model), half),
            vmem((2, share, model), half),
            vmem((share, model), half),
            vmem((share, model), half),
            vmem((share, model), half),
            vmem((n_fs, 2, SEQ_LEN, model), half),
            vmem((n_fs, 2, SEQ_LEN, model), half),
            vmem((n_fs, 2, share, model), half),
            vmem((n_fs, 2, share, model), half),
            vmem((n_fs, share, model), half),
            vmem((n_fs, share, model), half),
            vmem((n_fs, share, model), half),
            dma((5 * CHUNKS,)),
            dma((n_fs, CHUNKS)),
            dma((3 * CHUNKS,)),
            dma((3 * CHUNKS,)),
            dma((3,)),
            dma((3,)),
            dma((3, 3)),
            dma((n_fs, 3)),
            dma((3, 3)),
            dma((3, 3)),
            dma((5, 3)),
            dma((5, 3)),
            dma((5, SPREAD)),
            dma((n_fs, SPREAD)),
            dma((3, n_fs, SPREAD)),
            dma((3, n_fs, SPREAD)),
            dma((1, n_fs, 2)),
            dma((1, n_fs, 2)),
            dma((n_fs, PARTS)),
            dma((n_fs, PARTS)),
            dma((n_fs, PARTS)),
            dma((n_fs, PARTS)),
            dma((3, PARTS)),
            dma((3, PARTS)),
        ],
        compiler_params=pltpu.CompilerParams(
            collective_id=0, has_side_effects=True, vmem_limit_bytes=56 * 2**20
        ),
    )(
        stream,
        mix_pre_gain,
        mix_post_gain,
        ffn_pre_gain,
        ffn_post_gain,
        w_outer_gate.T,
        w_inner_gate.T,
        w_value.T,
        w_mix_out,
        mix_taps,
        cut(w_linear.T),
        cut(w_gated.T),
        cut(w_down),
        ffn_taps,
        ffn_bias,
    )


def on_device(rep, n_fs, n_tp, *arrays):
    stream, w_value, w_linear = arrays[0], arrays[4], arrays[9]
    same = n_fs == n_tp == 2 * rep == 4
    whole = w_value.shape[0] % 128 == 0 and 2 * w_value.shape[1] % (CHUNKS * PACK) == 0
    even = w_linear.shape[1] % (8 * n_fs) == 0 and stream.shape[0] == 2 * SEQ_LEN
    if same and whole and even:
        return split_plan(n_fs, *arrays)
    return gather_plan(*arrays)


def solution(mesh):
    in_specs = (
        P(("rep", "fs"), None),
        P(),
        P("fs", "tp"),
        P("fs", "tp"),
        P("fs", "tp"),
        P(None, "tp"),
        P("tp", "fs"),
        P(),
        P(),
        P("fs", "tp"),
        P("fs", "tp"),
        P(None, "tp"),
        P("tp"),
        P("tp", "fs"),
        P(),
    )
    out_specs = P(("rep", "fs"), None)
    sizes = mesh.shape
    body = functools.partial(on_device, sizes["rep"], sizes["fs"], sizes["tp"])
    return jax.shard_map(
        body, mesh=mesh, in_specs=in_specs, out_specs=out_specs, check_vma=False
    )
```

```python
import contextlib
import functools

import jax
import jax.numpy as jnp
from jax import lax
from jax.experimental import pallas as pl
from jax.experimental.pallas import tpu as pltpu
from jax.sharding import PartitionSpec as P

SEQ_LEN = 128
PACK = 16
CHUNKS = 4
SPREAD = 2
PARTS = 4
JOIN = 2
EDGE = (
    (),
    (),
    ((3, 0), (3, 1), (3, 2), (1, 0)),
    ((1, 1), (1, 2), (2, 0), (2, 1), (2, 2)),
)
INNER = (
    ((1, 0), (1, 1), (1, 2)),
    (),
    ((3, 0), (3, 1), (3, 2)),
    ((2, 0), (2, 1), (2, 2)),
)
TRACE = False


EPS = 1e-06


def norm_scale(values, gain):
    return values * lax.rsqrt(jnp.mean(values * values, axis=-1, keepdims=True) + EPS) * gain


def conv_three(values, taps):
    height, breadth = values.shape
    grouped = values.reshape(height // SEQ_LEN, SEQ_LEN, breadth)
    padded = jnp.pad(grouped, ((0, 0), (1, 1), (0, 0)))
    mixed = taps[0] * padded[:, :-2] + taps[1] * padded[:, 1:-1] + taps[2] * padded[:, 2:]
    return mixed.reshape(height, breadth)


def settle(partial_value, resid, post_gain):
    branch = lax.psum(partial_value.astype(jnp.bfloat16), "tp")
    return (resid + norm_scale(branch.astype(jnp.float32), post_gain)).astype(jnp.bfloat16)


def gather_plan(
    stream,
    mix_pre_gain,
    w_outer_gate,
    w_inner_gate,
    w_value,
    mix_taps,
    w_mix_out,
    mix_post_gain,
    ffn_pre_gain,
    w_linear,
    w_gated,
    ffn_taps,
    ffn_bias,
    w_down,
    ffn_post_gain,
):
    resid = stream.astype(jnp.float32)
    normed = norm_scale(resid, mix_pre_gain).astype(jnp.bfloat16)
    full_outer, full_inner, full_value = (
        lax.all_gather(w_outer_gate, "fs", axis=0, tiled=True),
        lax.all_gather(w_inner_gate, "fs", axis=0, tiled=True),
        lax.all_gather(w_value, "fs", axis=0, tiled=True),
    )
    outer = jnp.dot(normed, full_outer, preferred_element_type=jnp.float32)
    inner = jnp.dot(normed, full_inner, preferred_element_type=jnp.float32)
    value = jnp.dot(normed, full_value, preferred_element_type=jnp.float32)
    outer = outer.astype(jnp.bfloat16)
    inner = inner.astype(jnp.bfloat16)
    value = value.astype(jnp.bfloat16)
    product = inner.astype(jnp.float32) * value.astype(jnp.float32)
    mixed = (outer.astype(jnp.float32) * conv_three(product, mix_taps)).astype(jnp.bfloat16)
    full_mix_out = lax.all_gather(w_mix_out, "fs", axis=1, tiled=True)
    partial_value = jnp.dot(mixed, full_mix_out, preferred_element_type=jnp.float32)
    middle = settle(partial_value, resid, mix_post_gain)
    middle_f = middle.astype(jnp.float32)
    normed_two = norm_scale(middle_f, ffn_pre_gain).astype(jnp.bfloat16)
    full_linear, full_gated = (
        lax.all_gather(w_linear, "fs", axis=0, tiled=True),
        lax.all_gather(w_gated, "fs", axis=0, tiled=True),
    )
    linear = jnp.dot(normed_two, full_linear, preferred_element_type=jnp.float32)
    gated = jnp.dot(normed_two, full_gated, preferred_element_type=jnp.float32)
    linear = linear.astype(jnp.bfloat16)
    gated = gated.astype(jnp.bfloat16)
    activated = jax.nn.gelu(
        conv_three(gated.astype(jnp.float32), ffn_taps) + ffn_bias, approximate=True
    )
    hidden = (activated * linear.astype(jnp.float32)).astype(jnp.bfloat16)
    full_down = lax.all_gather(w_down, "fs", axis=1, tiled=True)
    partial_two = jnp.dot(hidden, full_down, preferred_element_type=jnp.float32)
    return settle(partial_two, middle_f, ffn_post_gain)


def dot_nt(left, right):
    return lax.dot_general(left, right, (((1,), (1,)), ((), ())), preferred_element_type=jnp.float32)


def dot_nn(left, right):
    return jnp.dot(left, right, preferred_element_type=jnp.float32)


def conv_rows(values, taps):
    height = values.shape[0]
    row = lax.broadcasted_iota(jnp.int32, values.shape, 0) % SEQ_LEN
    before = jnp.where(row == 0, 0.0, pltpu.roll(values, 1, 0))
    after = jnp.where(row == SEQ_LEN - 1, 0.0, pltpu.roll(values, height - 1, 0))
    return taps[0:1] * before + taps[1:2] * values + taps[2:3] * after


def norm_rows(values, gain):
    scale = lax.rsqrt(jnp.mean(values * values, axis=-1, keepdims=True) + EPS)
    return values * scale * gain


def scope(name):
    return jax.named_scope(name) if TRACE else contextlib.nullcontext()


def kernel(n_fs, conv_w, spans, *refs):
    sources, out, scratch = refs[:15], refs[15], refs[16:]
    (
        stream,
        gain_mix_pre,
        gain_mix_post,
        gain_ffn_pre,
        gain_ffn_post,
        mix_taps,
        w_linear,
        w_gated,
        w_down,
        ffn_taps,
        ffn_bias,
        load_s,
        small_all,
        smalls,
        ffn_w,
        ffn_all,
        mix_all,
        normed,
        acc,
        pm,
        rm,
        sm,
        rxm,
        middle,
        xs,
        pf,
        rf,
        sf,
        rx,
        tf,
        rz,
        rq,
        mz_s,
        mz_r,
        my_s,
        my_r,
        mr_s,
        mr_r,
        fz_s,
        fz_r,
        fy_s,
        fy_r,
        fx_s,
        fx_r,
        az_s,
        az_r,
        ap_s,
        ap_r,
        rs_s,
        rs_r,
        rp_s,
        rp_r,
        rz_s,
        rz_r,
        rq_r,
        fin_s,
        fin_r,
    ) = scratch
    r, f, t = lax.axis_index("rep"), lax.axis_index("fs"), lax.axis_index("tp")
    x, c = t // 2, t % 2
    t_core, t_side = 2 * x + 1 - c, 2 * (1 - x) + c
    core, side, other = {"tp": t_core}, {"tp": t_side}, {"rep": 1 - r}
    rows, width = stream.shape[0], ffn_w.shape[3]
    cap, few = ffn_w.shape[2], spans[0][1]
    sizes = (few, cap)
    share = rows // 4
    mine = pl.ds(pl.multiple_of(c * share, share), share)
    theirs = pl.ds(pl.multiple_of((1 - c) * share, share), share)

    near = f < n_fs // 2
    mirror = lambda v: jnp.where(near, v, n_fs - 1 - v)
    inner = jnp.where(near, f, n_fs - 1 - f) == 1
    edge = jnp.logical_not(inner)
    order = [mirror(jnp.where(inner, 0, 1)), mirror(2), mirror(3)]
    goals = [mirror(jnp.where(inner, 2, 1)), mirror(jnp.where(inner, 3, 2)), mirror(jnp.where(inner, 0, 3))]
    upward, downward = mirror(jnp.where(inner, 2, 1)), mirror(0)
    places = [f] + order

    started = []

    def send(src, dst, ss, rs, where):
        return pltpu.make_async_remote_copy(
            src_ref=src,
            dst_ref=dst,
            send_sem=ss,
            recv_sem=rs,
            device_id=where,
            device_id_type=pl.DeviceIdType.MESH,
        )

    def start(copy, when=None):
        started.append((copy, when))
        if when is None:
            copy.start()
        else:
            pl.when(when)(copy.start)

    def flush(count=None):
        with scope("sends"):
            for copy, when in started[:count]:
                if when is None:
                    copy.wait_send()
                else:
                    pl.when(when)(copy.wait_send)
        del started[:count]

    def wait(copy, name):
        with scope(name):
            copy.wait_recv()

    barrier = pltpu.get_barrier_semaphore()
    peers = [core, side, other] + [{"fs": (f + k) % n_fs} for k in (1, 2, 3)]
    for peer in peers:
        pl.semaphore_signal(barrier, inc=1, device_id=peer, device_id_type=pl.DeviceIdType.MESH)
    targets = [mix_all.at[f, p * conv_w : (p + 1) * conv_w] for p in range(4)]
    targets += [stream, gain_mix_pre, w_linear, w_gated, w_down, ffn_taps, ffn_bias]
    targets += [gain_mix_post, gain_ffn_pre, gain_ffn_post, mix_taps]
    places_in = (5, 6, 7, 8, 0, 1, 10, 11, 12, 13, 14, 2, 3, 4, 9)
    loads = [pltpu.make_async_copy(sources[i], ref, load_s.at[i]) for i, ref in zip(places_in, targets)]
    for load in loads:
        load.start()
    for load in loads[:4]:
        load.wait()
    with scope("barrier"):
        pl.semaphore_wait(barrier, len(peers))

    mix_half = mix_all.shape[1] // 2
    mix_cut = mix_half // CHUNKS

    def mix_copy(b, h, slot, to):
        at = pl.ds(pl.multiple_of(r * mix_half + h * mix_cut, PACK), mix_cut)
        ref = mix_all.at[b, at]
        return send(ref, ref, mz_s.at[slot], mz_r.at[b, h], {"fs": to})

    for h in range(CHUNKS):
        start(mix_copy(f, h, h, upward))
        start(mix_copy(f, h, CHUNKS + h, downward), inner)

    for load in loads[6:]:
        load.wait()

    pieces = (w_linear, w_gated, w_down)

    def keep(ref, at, size, piece):
        ref[0:size] = piece[at : at + size]
        if size < cap:
            ref[size:cap] = jnp.zeros((cap - size, width), ffn_w.dtype)

    for half in range(2):

        @pl.when(r == half)
        def _():
            for j, (at, *both) in enumerate(spans):
                for p, piece in enumerate(pieces):
                    keep(ffn_w.at[j, p], at + half * both[0], both[half], piece)

    narrow = ((cap, cap, few), (cap, few, few))

    def ffn_send(kind, i):
        for p in range(3):
            at = slice(0, narrow[kind][i])
            src, dst = ffn_w.at[goals[i], p, at], ffn_all.at[f, 0, p, at]
            yield send(src, dst, fz_s.at[i, p], fz_r.at[f, p], {"fs": goals[i]})

    kinds = (edge, inner)
    ffn_out = [[list(ffn_send(kind, i)) for i in range(3)] for kind in range(2)]
    for kind in range(2):
        started.extend((copy, kinds[kind]) for copies in ffn_out[kind] for copy in copies)

    def ffn_start(kind, *which):
        for i in which:
            for copy in ffn_out[kind][i]:
                copy.start()

    pl.when(edge)(functools.partial(ffn_start, 0, 0, 1, 2))

    own_side = [send(ffn_w.at[f, p], ffn_all.at[f, 2, p], fx_s.at[0, p], fx_r.at[0, p], side) for p in range(3)]
    for copy in own_side:
        start(copy)
    for p in range(3):
        ffn_all[f, 0, p] = ffn_w[f, p]
    for j, (at, *both) in enumerate(spans):
        for half in range(2):

            @pl.when((f == j) & (r == half))
            def _():
                for p, piece in enumerate(pieces):
                    keep(ffn_all.at[j, 1, p], at + (1 - half) * both[0], both[1 - half], piece)

    @pl.when(edge)
    def _():
        for i in range(1, 4):
            ffn_all[places[i], :, :, few:cap] = jnp.zeros((3, 3, cap - few, width), ffn_w.dtype)

    small_all[...] = jnp.zeros(small_all.shape, jnp.float32)
    for j, (first, *both) in enumerate(spans):
        for half, size in enumerate(both):
            at = first + half * both[0]
            small_all[j, half, 0:3, 0:size] = ffn_taps[:, at : at + size]
            small_all[j, half, 3:4, 0:size] = ffn_bias[at : at + size][None]
    smalls[0] = small_all[f, r]
    smalls[1] = small_all[f, 1 - r]
    small_copy = send(smalls.at[0], smalls.at[2], fx_s.at[4, 0], fx_r.at[4, 0], side)
    start(small_copy)

    for load in loads[4:6]:
        load.wait()
    step_rows = 32

    @pl.loop(0, rows // step_rows)
    def _(i):
        at = pl.ds(pl.multiple_of(i * step_rows, step_rows), step_rows)
        value = norm_rows(stream[at].astype(jnp.float32), gain_mix_pre[...][None]).astype(jnp.bfloat16)
        for j in range(n_fs):
            normed[j, at] = value[:, j * width : (j + 1) * width]

    def project(z, first=False):
        for p in range(3):
            term = dot_nt(normed[z], mix_all[z, p * conv_w : (p + 1) * conv_w])
            acc[p] = term if first else acc[p] + term

    project(f, True)

    flows = [(i, h) for i in range(3) for h in range(CHUNKS)]
    turns = [(i, h) for h in range(CHUNKS) for i in range(2)] + [(2, h) for h in range(CHUNKS)]
    my = []
    for e in range(3 * CHUNKS):
        (i_edge, h_edge), (i_inner, h_inner) = flows[e], turns[e]
        b = jnp.where(inner, order[i_inner], order[i_edge])
        h = jnp.where(inner, h_inner, h_edge)
        onward = downward if i_inner > 0 else upward
        copy = mix_copy(b, h, 2 * CHUNKS + e, onward)
        wait(copy, f"mixz_{e}")
        start(copy, inner)
        at = pl.ds(pl.multiple_of(r * mix_half + h * mix_cut, PACK), mix_cut)
        ref = mix_all.at[b, at]
        my.append(send(ref, ref, my_s.at[e], my_r.at[e], other))
        start(my[e])
        if e == 2 * CHUNKS - 2:
            pl.when(inner)(functools.partial(ffn_start, 1, 0, 1))
    pl.when(inner)(functools.partial(ffn_start, 1, 2))

    def hop(kind, i, p, piece, ss, rs, to):
        src = ffn_all.at[places[i], 0, p, 0 : sizes[kind]]
        dst = ffn_all.at[places[i], piece, p, 0 : sizes[kind]]
        return send(src, dst, ss.at[i, p], rs.at[i, p], to)

    trips = [(i, p) for i in range(1, 4) for p in range(3)]
    fy = [{(i, p): hop(kind, i, p, 1, fy_s, fy_r, other) for i, p in trips} for kind in range(2)]
    fx = [{(i, p): hop(kind, i, p, 2, fx_s, fx_r, side) for i, p in trips} for kind in range(2)]
    for kind in range(2):
        for group in (fy, fx):
            started.extend((copy, kinds[kind]) for copy in group[kind].values())

    def forward(kind, *which):
        for i, p in which:
            src = ffn_all.at[places[i], 0, p, 0 : sizes[kind]]
            wait(send(src, src, fz_s.at[i - 1, p], fz_r.at[places[i], p], other), f"ffnz_{i}_{p}")
            fy[kind][i, p].start()
            fx[kind][i, p].start()

    def relay(edge_list, inner_list):
        for kind, which in enumerate((edge_list, inner_list)):
            if which:
                pl.when(kinds[kind])(functools.partial(forward, kind, *which))

    def arrived(kind):
        for i, p in trips:
            wait(fy[kind][i, p], f"ffny_{i}_{p}")
            wait(fx[kind][i, p], f"ffnx_{i}_{p}")

    relay(EDGE[0], INNER[0])
    for e in range(3 * CHUNKS):
        if e == 3 * CHUNKS - 1:
            relay(EDGE[1], INNER[1])
        wait(my[e], f"mixy_{e}")
        if e == 2 * CHUNKS - 1:
            project(order[0])
            project(order[1])
    project(order[2])

    mix_core = []
    for k, q in enumerate((1 - x, x)):
        here = pl.ds(pl.multiple_of(q * SEQ_LEN, SEQ_LEN), SEQ_LEN)
        parts = [acc[p, here].astype(jnp.bfloat16).astype(jnp.float32) for p in range(3)]
        mixed = (parts[0] * conv_rows(parts[1] * parts[2], mix_taps)).astype(jnp.bfloat16)
        for j in range(n_fs):
            pm[k, :, j * width : (j + 1) * width] = dot_nn(
                mixed, mix_all[j, 3 * conv_w : 4 * conv_w]
            ).astype(jnp.bfloat16)
        mix_core.append(send(pm.at[k, theirs], rm.at[k], mr_s.at[k], mr_r.at[k], core))
        start(mix_core[k])

    def mix_sum(k):
        wait(mix_core[k], f"mixcore_{k}")
        return (pm[k, mine].astype(jnp.float32) + rm[k].astype(jnp.float32)).astype(jnp.bfloat16)

    sm[...] = mix_sum(0)
    mix_side = send(sm, rxm, mr_s.at[2], mr_r.at[2], side)
    start(mix_side)

    kept = mix_sum(1)
    relay(EDGE[2], INNER[2])
    wait(mix_side, "mixside")
    branch = (kept.astype(jnp.float32) + rxm[...].astype(jnp.float32)).astype(jnp.bfloat16)
    slot = pl.ds(pl.multiple_of(t * share, share), share)
    mid = stream[slot].astype(jnp.float32) + norm_rows(branch.astype(jnp.float32), gain_mix_post[...][None])
    mid = mid.astype(jnp.bfloat16)
    middle[...] = mid
    xs[f, 0, mine] = norm_rows(mid.astype(jnp.float32), gain_ffn_pre[...][None]).astype(jnp.bfloat16)

    sideways = [edge == (i % 2 == 1) for i in range(4)]
    partner = [{"rep": jnp.where(a, r, 1 - r), "tp": jnp.where(a, t_side, t)} for a in sideways]
    cut = share // SPREAD

    def piece_of(z, s, a):
        return xs.at[z, s, pl.ds(pl.multiple_of(c * share + a * cut, cut), cut)]

    ag_core, ag_pair, ag_pass = {}, {}, {}

    def line_copy(i, a):
        src = piece_of(places[i], 0, a)
        onward = downward if i > 1 else upward
        return send(src, src, az_s.at[1 + i, a], az_r.at[places[i], a], {"fs": onward})

    ag_line = {(i, a): line_copy(i, a) for i in range(1, 4) for a in range(SPREAD)}
    for i in range(4):
        for a in range(SPREAD):
            src = piece_of(places[i], 0, a)
            ag_pair[i, a] = send(src, piece_of(places[i], 1, a), ap_s.at[0, i, a], ap_r.at[0, i, a], partner[i])
            ag_core[i, a] = send(src, src, ap_s.at[1, i, a], ap_r.at[1, i, a], core)
            started.extend(((ag_pair[i, a], None), (ag_core[i, a], None)))
            if i > 0:
                started.append((ag_line[i, a], inner))

    def spread(i):
        for a in range(SPREAD):
            src = piece_of(places[i], 0, a)
            if i == 0:
                start(send(src, src, az_s.at[0, a], az_r.at[places[i], a], {"fs": upward}))
                start(send(src, src, az_s.at[1, a], az_r.at[places[i], a], {"fs": downward}), inner)
            else:
                wait(ag_line[i, a], f"agz_{i}_{a}")
                pl.when(inner)(ag_line[i, a].start)
            ag_pair[i, a].start()
            ag_core[i, a].start()

    for i in range(4):
        for a in range(SPREAD):
            src = piece_of(places[i], 1, a)
            ag_pass[i, a] = send(src, src, ap_s.at[2, i, a], ap_r.at[2, i, a], core)
            started.append((ag_pass[i, a], None))

    def pass_on(i):
        for a in range(SPREAD):
            wait(ag_pair[i, a], f"agpair_{i}_{a}")
            ag_pass[i, a].start()

    rs_core, rs_pair = {}, {}
    part = share // PARTS

    def block(i):
        for s in range(2):
            for a in range(SPREAD):
                wait((ag_pass if s else ag_core)[i, a], f"agcore_{i}_{s}_{a}")
        z = places[i]
        second = jnp.where(sideways[i], 1, 2)
        with scope(f"block_{i}"):
            hidden = []
            for h in (0, second):
                linear, gated = 0.0, 0.0
                for j in range(0, n_fs, JOIN):
                    act = xs[z, :, :, j * width : (j + JOIN) * width].reshape(2 * SEQ_LEN, JOIN * width)
                    joined = lambda p: jnp.concatenate([ffn_all[j + k, h, p] for k in range(JOIN)], axis=1)
                    linear = linear + dot_nt(act, joined(0))
                    gated = gated + dot_nt(act, joined(1))
                linear = linear.astype(jnp.bfloat16).astype(jnp.float32)
                gated = gated.astype(jnp.bfloat16).astype(jnp.float32)
                small = smalls[h]
                act = jax.nn.gelu(conv_rows(gated, small) + small[3:4], approximate=True)
                hidden.append((act * linear).astype(jnp.bfloat16))
            for j in range(n_fs):
                total = dot_nn(hidden[0], ffn_all[j, 0, 2]) + dot_nn(hidden[1], ffn_all[j, second, 2])
                total = total.astype(jnp.bfloat16).reshape(2, SEQ_LEN, width)
                pf[i, :, :, j * width : (j + 1) * width] = total
        for s in (1, 0):
            rs_core[i, s] = send(pf.at[i, s, theirs], rf.at[i, s], rs_s.at[0, i, s], rs_r.at[0, i, s], core)
            start(rs_core[i, s])

    def stage_core(i, s):
        wait(rs_core[i, s], f"rscore_{i}_{s}")
        for a in range(PARTS):
            at = pl.ds(a * part, part)
            ours = pl.ds(pl.multiple_of(c * share + a * part, part), part)
            total = pf[i, s, ours].astype(jnp.float32) + rf[i, s, at].astype(jnp.float32)
            sf[i, s, at] = total.astype(jnp.bfloat16)
            if s:
                rs_pair[i, a] = send(sf.at[i, s, at], rx.at[i, at], rp_s.at[i, a], rp_r.at[i, a], partner[i])
                start(rs_pair[i, a])

    rs_line, late = {}, []
    for i in range(1, 4):
        for a in range(PARTS):
            at = pl.ds(a * part, part)
            home = send(tf.at[i, at], rz.at[f, at], rz_s.at[i, a], rz_r.at[f, a], {"fs": places[i]})
            late.append((home, None if i == 1 else inner))
            rs_line[i, a] = home, None
            if i > 1:
                near_by = send(tf.at[i, at], rq.at[i, at], rz_s.at[i, a], rq_r.at[i, a], {"fs": places[1]})
                late.append((near_by, edge))
                rs_line[i, a] = home, near_by

    def stage_pair(i):
        for a in range(PARTS):
            at = pl.ds(a * part, part)
            wait(rs_pair[i, a], f"rspair_{i}_{a}")
            total = sf[i, 0, at].astype(jnp.float32) + rx[i, at].astype(jnp.float32)
            if i == 0:
                tf[i, at] = total.astype(jnp.bfloat16)
                continue
            home, near_by = rs_line[i, a]
            if near_by is None:
                tf[i, at] = total.astype(jnp.bfloat16)
                home.start()
                continue

            @pl.when(edge)
            def _():
                tf[i, at] = total.astype(jnp.bfloat16)
                near_by.start()

            @pl.when(inner)
            def _():
                wait(near_by, f"rq_{i}_{a}")
                tf[i, at] = (total + rq[i, at].astype(jnp.float32)).astype(jnp.bfloat16)
                home.start()

    def stage(i):
        stage_core(i, 1)
        stage_core(i, 0)

    spread(0)
    relay(EDGE[3], INNER[3])

    @pl.when(edge)
    def _():
        pass_on(0)
        spread(1)
        spread(2)
        arrived(0)

    @pl.when(inner)
    def _():
        spread(1)
        spread(2)
        spread(3)
        pass_on(0)
        arrived(1)

    for copy in own_side + [small_copy]:
        wait(copy, "ffnown")
    block(0)
    pass_on(1)
    pl.when(edge)(functools.partial(spread, 3))
    pass_on(2)
    early = len(started)
    block(1)
    block(2)
    stage(1)
    pass_on(3)
    stage(2)
    stage(0)
    block(3)
    stage(3)

    @pl.when(edge)
    def _():
        stage_pair(2)
        stage_pair(3)
        stage_pair(1)

    @pl.when(inner)
    def _():
        stage_pair(1)
        stage_pair(2)
        stage_pair(3)

    stage_pair(0)
    flush(early)
    started.extend(late)

    def row_slot(who, a):
        return pl.ds(pl.multiple_of(who * share + a * part, part), part)

    fin = {}
    for a in range(PARTS):
        at = pl.ds(a * part, part)
        total = tf[0, at].astype(jnp.float32)
        for i in range(1, 3):
            ref = rz.at[places[i], at]
            wait(send(ref, ref, rz_s.at[0, a], rz_r.at[places[i], a], {"fs": places[i]}), f"rz_{i}_{a}")
            total = total + rz[places[i], at].astype(jnp.float32)
        branch = total.astype(jnp.bfloat16).astype(jnp.float32)
        done = middle[at].astype(jnp.float32) + norm_rows(branch, gain_ffn_post[...][None])
        out[row_slot(t, a)] = done.astype(jnp.bfloat16)
        own = out.at[row_slot(t, a)]
        for k, to in enumerate((side, core)):
            fin[k, a] = send(own, own, fin_s.at[k, a], fin_r.at[k, a], to)
            start(fin[k, a])
    for a in range(PARTS):
        wait(fin[0, a], f"finside_{a}")
        far = out.at[row_slot(t_side, a)]
        fin[2, a] = send(far, far, fin_s.at[2, a], fin_r.at[2, a], core)
        start(fin[2, a])
    for a in range(PARTS):
        wait(fin[1, a], f"fincore_{a}")
        wait(fin[2, a], f"finpass_{a}")

    flush()


def split_plan(
    n_fs,
    stream,
    mix_pre_gain,
    w_outer_gate,
    w_inner_gate,
    w_value,
    mix_taps,
    w_mix_out,
    mix_post_gain,
    ffn_pre_gain,
    w_linear,
    w_gated,
    ffn_taps,
    ffn_bias,
    w_down,
    ffn_post_gain,
):
    rows, model = stream.shape
    width, conv_w = w_value.shape
    tiles = w_linear.shape[1] // (2 * PACK)
    few = tiles * 7 // 32 * PACK
    more = tiles * PACK - 2 * few
    cap = -(-more // (2 * PACK)) * PACK
    spans, at = [], 0
    for z in range(n_fs):
        both = (few, few) if z in (0, n_fs - 1) else (cap, more - cap)
        spans.append((at, *both))
        at += sum(both)
    share = rows // 4
    half = jnp.bfloat16
    vmem, dma = pltpu.VMEM, pltpu.SemaphoreType.DMA
    return pl.pallas_call(
        functools.partial(kernel, n_fs, conv_w, tuple(spans)),
        out_shape=pltpu.VMEM((rows, model), half),
        in_specs=[pl.BlockSpec(memory_space=pltpu.HBM)] * 15,
        out_specs=pl.BlockSpec(memory_space=vmem),
        scratch_shapes=[
            vmem((rows, model), half),
            vmem((model,), jnp.float32),
            vmem((model,), jnp.float32),
            vmem((model,), jnp.float32),
            vmem((model,), jnp.float32),
            vmem(mix_taps.shape, jnp.float32),
            vmem(w_down.shape, half),
            vmem(w_down.shape, half),
            vmem(w_down.shape, half),
            vmem(ffn_taps.shape, jnp.float32),
            vmem(ffn_bias.shape, jnp.float32),
            dma((15,)),
            vmem((n_fs, 2, 8, cap), jnp.float32),
            vmem((3, 8, cap), jnp.float32),
            vmem((n_fs, 3, cap, width), half),
            vmem((n_fs, 3, 3, cap, width), half),
            vmem((n_fs, 4 * conv_w, width), half),
            vmem((n_fs, rows, width), half),
            vmem((3, rows, conv_w), jnp.float32),
            vmem((2, SEQ_LEN, model), half),
            vmem((2, share, model), half),
            vmem((share, model), half),
            vmem((share, model), half),
            vmem((share, model), half),
            vmem((n_fs, 2, SEQ_LEN, model), half),
            vmem((n_fs, 2, SEQ_LEN, model), half),
            vmem((n_fs, 2, share, model), half),
            vmem((n_fs, 2, share, model), half),
            vmem((n_fs, share, model), half),
            vmem((n_fs, share, model), half),
            vmem((n_fs, share, model), half),
            vmem((n_fs, share, model), half),
            dma((5 * CHUNKS,)),
            dma((n_fs, CHUNKS)),
            dma((3 * CHUNKS,)),
            dma((3 * CHUNKS,)),
            dma((3,)),
            dma((3,)),
            dma((3, 3)),
            dma((n_fs, 3)),
            dma((n_fs, 3)),
            dma((n_fs, 3)),
            dma((5, 3)),
            dma((5, 3)),
            dma((5, SPREAD)),
            dma((n_fs, SPREAD)),
            dma((3, n_fs, SPREAD)),
            dma((3, n_fs, SPREAD)),
            dma((1, n_fs, 2)),
            dma((1, n_fs, 2)),
            dma((n_fs, PARTS)),
            dma((n_fs, PARTS)),
            dma((n_fs, PARTS)),
            dma((n_fs, PARTS)),
            dma((n_fs, PARTS)),
            dma((3, PARTS)),
            dma((3, PARTS)),
        ],
        compiler_params=pltpu.CompilerParams(
            collective_id=0, has_side_effects=True, vmem_limit_bytes=58 * 2**20
        ),
    )(
        stream,
        mix_pre_gain,
        mix_post_gain,
        ffn_pre_gain,
        ffn_post_gain,
        w_outer_gate.T,
        w_inner_gate.T,
        w_value.T,
        w_mix_out,
        mix_taps,
        w_linear.T,
        w_gated.T,
        w_down,
        ffn_taps,
        ffn_bias,
    )


def on_device(rep, n_fs, n_tp, *arrays):
    stream, w_value, w_linear = arrays[0], arrays[4], arrays[9]
    same = n_fs == n_tp == 2 * rep == 4
    whole = w_value.shape[0] % 128 == 0 and 2 * w_value.shape[1] % (CHUNKS * PACK) == 0
    even = w_linear.shape[1] % (2 * PACK) == 0 and stream.shape[0] == 2 * SEQ_LEN
    if same and whole and even:
        return split_plan(n_fs, *arrays)
    return gather_plan(*arrays)


def solution(mesh):
    in_specs = (
        P(("rep", "fs"), None),
        P(),
        P("fs", "tp"),
        P("fs", "tp"),
        P("fs", "tp"),
        P(None, "tp"),
        P("tp", "fs"),
        P(),
        P(),
        P("fs", "tp"),
        P("fs", "tp"),
        P(None, "tp"),
        P("tp"),
        P("tp", "fs"),
        P(),
    )
    out_specs = P(("rep", "fs"), None)
    sizes = mesh.shape
    body = functools.partial(on_device, sizes["rep"], sizes["fs"], sizes["tp"])
    return jax.shard_map(
        body, mesh=mesh, in_specs=in_specs, out_specs=out_specs, check_vma=False
    )
```

```python
import contextlib
import functools

import jax
import jax.numpy as jnp
from jax import lax
from jax.experimental import pallas as pl
from jax.experimental.pallas import tpu as pltpu
from jax.sharding import PartitionSpec as P

SEQ_LEN = 128
PACK = 16
CHUNKS = 4
SPREAD = 2
PARTS = 4
JOIN = 2
FIRST = (0, 1)
EDGE = (
    (),
    (),
    ((3, 0), (3, 1), (3, 2), (1, 0)),
    ((1, 1), (1, 2), (2, 0), (2, 1), (2, 2)),
)
INNER = (
    ((1, 0), (1, 1), (1, 2)),
    ((3, 0), (3, 1)),
    ((3, 2), (2, 0), (2, 1)),
    ((2, 2),),
)
SIDEWAYS = ((True, False, False, True), (True, True, True, False))
TRACE = False


EPS = 1e-06


def norm_scale(values, gain):
    return values * lax.rsqrt(jnp.mean(values * values, axis=-1, keepdims=True) + EPS) * gain


def conv_three(values, taps):
    height, breadth = values.shape
    grouped = values.reshape(height // SEQ_LEN, SEQ_LEN, breadth)
    padded = jnp.pad(grouped, ((0, 0), (1, 1), (0, 0)))
    mixed = taps[0] * padded[:, :-2] + taps[1] * padded[:, 1:-1] + taps[2] * padded[:, 2:]
    return mixed.reshape(height, breadth)


def settle(partial_value, resid, post_gain):
    branch = lax.psum(partial_value.astype(jnp.bfloat16), "tp")
    return (resid + norm_scale(branch.astype(jnp.float32), post_gain)).astype(jnp.bfloat16)


def gather_plan(
    stream,
    mix_pre_gain,
    w_outer_gate,
    w_inner_gate,
    w_value,
    mix_taps,
    w_mix_out,
    mix_post_gain,
    ffn_pre_gain,
    w_linear,
    w_gated,
    ffn_taps,
    ffn_bias,
    w_down,
    ffn_post_gain,
):
    resid = stream.astype(jnp.float32)
    normed = norm_scale(resid, mix_pre_gain).astype(jnp.bfloat16)
    full_outer, full_inner, full_value = (
        lax.all_gather(w_outer_gate, "fs", axis=0, tiled=True),
        lax.all_gather(w_inner_gate, "fs", axis=0, tiled=True),
        lax.all_gather(w_value, "fs", axis=0, tiled=True),
    )
    outer = jnp.dot(normed, full_outer, preferred_element_type=jnp.float32)
    inner = jnp.dot(normed, full_inner, preferred_element_type=jnp.float32)
    value = jnp.dot(normed, full_value, preferred_element_type=jnp.float32)
    outer = outer.astype(jnp.bfloat16)
    inner = inner.astype(jnp.bfloat16)
    value = value.astype(jnp.bfloat16)
    product = inner.astype(jnp.float32) * value.astype(jnp.float32)
    mixed = (outer.astype(jnp.float32) * conv_three(product, mix_taps)).astype(jnp.bfloat16)
    full_mix_out = lax.all_gather(w_mix_out, "fs", axis=1, tiled=True)
    partial_value = jnp.dot(mixed, full_mix_out, preferred_element_type=jnp.float32)
    middle = settle(partial_value, resid, mix_post_gain)
    middle_f = middle.astype(jnp.float32)
    normed_two = norm_scale(middle_f, ffn_pre_gain).astype(jnp.bfloat16)
    full_linear, full_gated = (
        lax.all_gather(w_linear, "fs", axis=0, tiled=True),
        lax.all_gather(w_gated, "fs", axis=0, tiled=True),
    )
    linear = jnp.dot(normed_two, full_linear, preferred_element_type=jnp.float32)
    gated = jnp.dot(normed_two, full_gated, preferred_element_type=jnp.float32)
    linear = linear.astype(jnp.bfloat16)
    gated = gated.astype(jnp.bfloat16)
    activated = jax.nn.gelu(
        conv_three(gated.astype(jnp.float32), ffn_taps) + ffn_bias, approximate=True
    )
    hidden = (activated * linear.astype(jnp.float32)).astype(jnp.bfloat16)
    full_down = lax.all_gather(w_down, "fs", axis=1, tiled=True)
    partial_two = jnp.dot(hidden, full_down, preferred_element_type=jnp.float32)
    return settle(partial_two, middle_f, ffn_post_gain)


def dot_nt(left, right):
    return lax.dot_general(left, right, (((1,), (1,)), ((), ())), preferred_element_type=jnp.float32)


def dot_nn(left, right):
    return jnp.dot(left, right, preferred_element_type=jnp.float32)


def conv_rows(values, taps):
    height = values.shape[0]
    row = lax.broadcasted_iota(jnp.int32, values.shape, 0) % SEQ_LEN
    before = jnp.where(row == 0, 0.0, pltpu.roll(values, 1, 0))
    after = jnp.where(row == SEQ_LEN - 1, 0.0, pltpu.roll(values, height - 1, 0))
    return taps[0:1] * before + taps[1:2] * values + taps[2:3] * after


def norm_rows(values, gain):
    scale = lax.rsqrt(jnp.mean(values * values, axis=-1, keepdims=True) + EPS)
    return values * scale * gain


def scope(name):
    return jax.named_scope(name) if TRACE else contextlib.nullcontext()


def kernel(n_fs, conv_w, spans, *refs):
    sources, out, scratch = refs[:15], refs[15], refs[16:]
    (
        stream,
        gain_mix_pre,
        gain_mix_post,
        gain_ffn_pre,
        gain_ffn_post,
        mix_taps,
        w_linear,
        w_gated,
        w_down,
        ffn_taps,
        ffn_bias,
        load_s,
        small_all,
        smalls,
        ffn_w,
        ffn_all,
        mix_all,
        normed,
        acc,
        pm,
        rm,
        sm,
        rxm,
        middle,
        xs,
        pf,
        rf,
        sf,
        rx,
        tf,
        rz,
        rq,
        mz_s,
        mz_r,
        my_s,
        my_r,
        mr_s,
        mr_r,
        fz_s,
        fz_r,
        fy_s,
        fy_r,
        fx_s,
        fx_r,
        az_s,
        az_r,
        ap_s,
        ap_r,
        ac_r,
        rs_s,
        rs_r,
        rp_r,
        rz_r,
        rq_r,
        fin_s,
        fin_r,
    ) = scratch
    r, f, t = lax.axis_index("rep"), lax.axis_index("fs"), lax.axis_index("tp")
    x, c = t // 2, t % 2
    t_core, t_side = 2 * x + 1 - c, 2 * (1 - x) + c
    core, side, other = {"tp": t_core}, {"tp": t_side}, {"rep": 1 - r}
    rows, width = stream.shape[0], ffn_w.shape[3]
    cap, few = ffn_w.shape[2], spans[0][1]
    sizes = (few, cap)
    share = rows // 4
    mine = pl.ds(pl.multiple_of(c * share, share), share)
    theirs = pl.ds(pl.multiple_of((1 - c) * share, share), share)

    near = f < n_fs // 2
    mirror = lambda v: jnp.where(near, v, n_fs - 1 - v)
    inner = jnp.where(near, f, n_fs - 1 - f) == 1
    edge = jnp.logical_not(inner)
    order = [mirror(jnp.where(inner, 0, 1)), mirror(2), mirror(3)]
    goals = [mirror(jnp.where(inner, 2, 1)), mirror(jnp.where(inner, 3, 2)), mirror(jnp.where(inner, 0, 3))]
    upward, downward = mirror(jnp.where(inner, 2, 1)), mirror(0)
    places = [f] + order

    def send(src, dst, ss, rs, where):
        return pltpu.make_async_remote_copy(
            src_ref=src,
            dst_ref=dst,
            send_sem=ss,
            recv_sem=rs,
            device_id=where,
            device_id_type=pl.DeviceIdType.MESH,
        )

    owed = []

    def owe(ref, sem, when=None):
        owed.append((send(ref, ref, sem, sem, core), when))

    def settle_sends():
        for copy, when in owed:
            if when is None:
                copy.wait_send()
            else:
                pl.when(when)(copy.wait_send)

    def begin(copy, when=None):
        if when is None:
            copy.start()
        else:
            pl.when(when)(copy.start)

    def landed(ref, sem, name):
        wait(send(ref, ref, sem, sem, core), name)

    def wait(copy, name):
        with scope(name):
            copy.wait_recv()

    barrier = pltpu.get_barrier_semaphore()
    peers = [core, side, other] + [{"fs": (f + k) % n_fs} for k in (1, 2, 3)]
    for peer in peers:
        pl.semaphore_signal(barrier, inc=1, device_id=peer, device_id_type=pl.DeviceIdType.MESH)
    targets = [mix_all.at[f, p * conv_w : (p + 1) * conv_w] for p in range(4)]
    targets += [stream, gain_mix_pre, w_linear, w_gated, w_down, ffn_taps, ffn_bias]
    targets += [gain_mix_post, gain_ffn_pre, gain_ffn_post, mix_taps]
    places_in = (5, 6, 7, 8, 0, 1, 10, 11, 12, 13, 14, 2, 3, 4, 9)
    loads = [
        pltpu.make_async_copy(sources[i], ref, load_s.at[max(k - 3, 0)])
        for k, (i, ref) in enumerate(zip(places_in, targets))
    ]
    for load in loads:
        load.start()
    pltpu.make_async_copy(mix_all.at[f], mix_all.at[f], load_s.at[0]).wait()
    with scope("barrier"):
        pl.semaphore_wait(barrier, len(peers))

    mix_half = mix_all.shape[1] // 2
    mix_cut = mix_half // CHUNKS

    def mix_copy(b, h, to):
        at = pl.ds(pl.multiple_of(r * mix_half + h * mix_cut, PACK), mix_cut)
        ref = mix_all.at[b, at]
        return send(ref, ref, mz_s.at[0], mz_r.at[b, h], {"fs": to})

    for h in range(CHUNKS):
        begin(mix_copy(f, h, upward))
        begin(mix_copy(f, h, downward), inner)
    owe(mix_all.at[0, 0:mix_half], mz_s.at[0], edge)
    owe(mix_all.at[0:n_fs, 0 : mix_half * 5 // n_fs], mz_s.at[0], inner)

    for load in loads[6:]:
        load.wait()

    pieces = (w_linear, w_gated, w_down)

    def keep(ref, at, size, piece):
        ref[0:size] = piece[at : at + size]
        if size < cap:
            ref[size:cap] = jnp.zeros((cap - size, width), ffn_w.dtype)

    for half in range(2):

        @pl.when(r == half)
        def _():
            for j, (at, *both) in enumerate(spans):
                for p, piece in enumerate(pieces):
                    keep(ffn_w.at[j, p], at + half * both[0], both[half], piece)

    narrow = ((cap, cap, few), (cap, few, few))

    def ffn_send(kind, i):
        for p in range(3):
            at = slice(0, narrow[kind][i])
            src, dst = ffn_w.at[goals[i], p, at], ffn_all.at[f, 0, p, at]
            yield send(src, dst, fz_s.at[i], fz_r.at[f, p], {"fs": goals[i]})

    kinds = (edge, inner)
    ffn_out = [[list(ffn_send(kind, i)) for i in range(3)] for kind in range(2)]
    for kind in range(2):
        for i in range(3):
            owe(ffn_w.at[0, :, 0 : narrow[kind][i]], fz_s.at[i], kinds[kind])

    def ffn_start(kind, *which):
        for i in which:
            for copy in ffn_out[kind][i]:
                copy.start()

    pl.when(edge)(functools.partial(ffn_start, 0, 0, 1, 2))

    own_side = send(ffn_w.at[f], ffn_all.at[f, 2], fx_s.at[0], fx_r.at[0], side)
    own_side.start()
    owe(ffn_w.at[f], fx_s.at[0])
    for p in range(3):
        ffn_all[f, 0, p] = ffn_w[f, p]
    for j, (at, *both) in enumerate(spans):
        for half in range(2):

            @pl.when((f == j) & (r == half))
            def _():
                for p, piece in enumerate(pieces):
                    keep(ffn_all.at[j, 1, p], at + (1 - half) * both[0], both[1 - half], piece)

    @pl.when(edge)
    def _():
        for i in range(1, 4):
            ffn_all[places[i], :, :, few:cap] = jnp.zeros((3, 3, cap - few, width), ffn_w.dtype)

    small_all[...] = jnp.zeros(small_all.shape, jnp.float32)
    for j, (first, *both) in enumerate(spans):
        for half, size in enumerate(both):
            at = first + half * both[0]
            small_all[j, half, 0:3, 0:size] = ffn_taps[:, at : at + size]
            small_all[j, half, 3:4, 0:size] = ffn_bias[at : at + size][None]
    smalls[0] = small_all[f, r]
    smalls[1] = small_all[f, 1 - r]
    small_copy = send(smalls.at[0], smalls.at[2], fx_s.at[1], fx_r.at[1], side)
    small_copy.start()
    owe(smalls.at[0], fx_s.at[1])

    for load in loads[4:6]:
        load.wait()
    step_rows = 32

    @pl.loop(0, rows // step_rows)
    def _(i):
        at = pl.ds(pl.multiple_of(i * step_rows, step_rows), step_rows)
        value = norm_rows(stream[at].astype(jnp.float32), gain_mix_pre[...][None]).astype(jnp.bfloat16)
        for j in range(n_fs):
            normed[j, at] = value[:, j * width : (j + 1) * width]

    def project(z, first=False):
        for p in range(3):
            term = dot_nt(normed[z], mix_all[z, p * conv_w : (p + 1) * conv_w])
            acc[p] = term if first else acc[p] + term

    project(f, True)

    flows = [(i, h) for i in range(3) for h in range(CHUNKS)]
    turns = [(i, h) for h in range(CHUNKS) for i in range(2)] + [(2, h) for h in range(CHUNKS)]
    my = []
    for e in range(3 * CHUNKS):
        (i_edge, h_edge), (i_inner, h_inner) = flows[e], turns[e]
        b = jnp.where(inner, order[i_inner], order[i_edge])
        h = jnp.where(inner, h_inner, h_edge)
        onward = downward if i_inner > 0 else upward
        copy = mix_copy(b, h, onward)
        wait(copy, f"mixz_{e}")
        begin(copy, inner)
        at = pl.ds(pl.multiple_of(r * mix_half + h * mix_cut, PACK), mix_cut)
        ref = mix_all.at[b, at]
        my.append(send(ref, ref, my_s.at[0], my_r.at[e], other))
        my[e].start()
        if e == 2 * CHUNKS - 2:
            pl.when(inner)(functools.partial(ffn_start, 1, *FIRST))
    owe(mix_all.at[0:3, 0:mix_half], my_s.at[0])
    pl.when(inner)(functools.partial(ffn_start, 1, 2))

    def hop(kind, i, p, piece, ss, rs, to):
        src = ffn_all.at[places[i], 0, p, 0 : sizes[kind]]
        dst = ffn_all.at[places[i], piece, p, 0 : sizes[kind]]
        return send(src, dst, ss, rs, to)

    trips = [(i, p) for i in range(1, 4) for p in range(3)]
    fy = [{(i, p): hop(kind, i, p, 1, fy_s.at[0], fy_r.at[0], other) for i, p in trips} for kind in range(2)]
    fx = [{(i, p): hop(kind, i, p, 2, fx_s.at[2], fx_r.at[2], side) for i, p in trips} for kind in range(2)]
    all_trips = [ffn_all.at[0:3, 0, :, 0 : sizes[kind]] for kind in range(2)]
    for kind in range(2):
        owe(all_trips[kind], fy_s.at[0], kinds[kind])
        owe(all_trips[kind], fx_s.at[2], kinds[kind])

    def forward(kind, *which):
        for i, p in which:
            src = ffn_all.at[places[i], 0, p, 0 : sizes[kind]]
            wait(send(src, src, fz_s.at[i - 1], fz_r.at[places[i], p], other), f"ffnz_{i}_{p}")
            fy[kind][i, p].start()
            fx[kind][i, p].start()

    def relay(edge_list, inner_list):
        for kind, which in enumerate((edge_list, inner_list)):
            if which:
                pl.when(kinds[kind])(functools.partial(forward, kind, *which))

    def arrived(kind):
        landed(all_trips[kind], fy_r.at[0], "ffny")
        landed(all_trips[kind], fx_r.at[2], "ffnx")

    relay(EDGE[0], INNER[0])
    for e in range(3 * CHUNKS):
        if e == 2 * CHUNKS:
            relay(EDGE[1], INNER[1])
        wait(my[e], f"mixy_{e}")
        if e == 2 * CHUNKS - 1:
            project(order[0])
            project(order[1])
    project(order[2])

    mix_core = []
    for k, q in enumerate((1 - x, x)):
        here = pl.ds(pl.multiple_of(q * SEQ_LEN, SEQ_LEN), SEQ_LEN)
        parts = [acc[p, here].astype(jnp.bfloat16).astype(jnp.float32) for p in range(3)]
        mixed = (parts[0] * conv_rows(parts[1] * parts[2], mix_taps)).astype(jnp.bfloat16)
        for j in range(n_fs):
            pm[k, :, j * width : (j + 1) * width] = dot_nn(
                mixed, mix_all[j, 3 * conv_w : 4 * conv_w]
            ).astype(jnp.bfloat16)
        mix_core.append(send(pm.at[k, theirs], rm.at[k], mr_s.at[0], mr_r.at[k], core))
        mix_core[k].start()

    def mix_sum(k):
        wait(mix_core[k], f"mixcore_{k}")
        return (pm[k, mine].astype(jnp.float32) + rm[k].astype(jnp.float32)).astype(jnp.bfloat16)

    sm[...] = mix_sum(0)
    mix_side = send(sm, rxm, mr_s.at[0], mr_r.at[2], side)
    mix_side.start()
    owe(rz.at[0:3], mr_s.at[0])

    kept = mix_sum(1)
    relay(EDGE[2], INNER[2])
    wait(mix_side, "mixside")
    branch = (kept.astype(jnp.float32) + rxm[...].astype(jnp.float32)).astype(jnp.bfloat16)
    slot = pl.ds(pl.multiple_of(t * share, share), share)
    mid = stream[slot].astype(jnp.float32) + norm_rows(branch.astype(jnp.float32), gain_mix_post[...][None])
    mid = mid.astype(jnp.bfloat16)
    middle[...] = mid
    xs[f, 0, mine] = norm_rows(mid.astype(jnp.float32), gain_ffn_pre[...][None]).astype(jnp.bfloat16)

    sideways = [jnp.where(edge, a, b) for a, b in zip(*SIDEWAYS)]
    partner = [{"rep": jnp.where(a, r, 1 - r), "tp": jnp.where(a, t_side, t)} for a in sideways]
    cut = share // SPREAD

    def piece_of(z, s, a):
        return xs.at[z, s, pl.ds(pl.multiple_of(c * share + a * cut, cut), cut)]

    ag_core, ag_pair, ag_pass = {}, {}, {}

    slab = pl.ds(pl.multiple_of(c * share, share), share)
    slab_core = pl.ds(pl.multiple_of((1 - c) * share, share), share)
    for i in range(4):
        for a in range(SPREAD):
            src, far = piece_of(places[i], 0, a), piece_of(places[i], 1, a)
            ag_pair[i, a] = send(src, far, ap_s.at[0], ap_r.at[i, a], partner[i])
            ag_core[i, a] = send(src, src, ap_s.at[1], ac_r.at[0, i], core)
            ag_pass[i, a] = send(far, far, ap_s.at[2], ac_r.at[1, i], core)
    for k in range(3):
        owe(rz, ap_s.at[k])
    owe(rz.at[0], az_s.at[0])
    owe(rz, az_s.at[1], inner)

    def pair_own():
        for a in range(SPREAD):
            ag_pair[0, a].start()

    def spread(i, which=range(SPREAD)):
        for a in which:
            src = piece_of(places[i], 0, a)
            if i == 0:
                send(src, src, az_s.at[0], az_r.at[f, a], {"fs": upward}).start()
                begin(send(src, src, az_s.at[1], az_r.at[f, a], {"fs": downward}), inner)
            else:
                copy = send(src, src, az_s.at[1], az_r.at[places[i], a], {"fs": downward if i > 1 else upward})
                wait(copy, f"agz_{i}_{a}")
                begin(copy, inner)
                ag_pair[i, a].start()
            ag_core[i, a].start()

    def pass_on(i):
        for a in range(SPREAD):
            wait(ag_pair[i, a], f"agpair_{i}_{a}")
            ag_pass[i, a].start()

    rs_core, rs_pair = {}, {}
    part = share // PARTS

    def block(i):
        for s in range(2):
            landed(xs.at[places[i], s, slab_core], ac_r.at[s, i], f"agcore_{i}_{s}")
        z = places[i]
        second = jnp.where(sideways[i], 1, 2)
        with scope(f"block_{i}"):
            hidden = []
            for h in (0, second):
                linear, gated = 0.0, 0.0
                for j in range(0, n_fs, JOIN):
                    act = xs[z, :, :, j * width : (j + JOIN) * width].reshape(2 * SEQ_LEN, JOIN * width)
                    joined = lambda p: jnp.concatenate([ffn_all[j + k, h, p] for k in range(JOIN)], axis=1)
                    linear = linear + dot_nt(act, joined(0))
                    gated = gated + dot_nt(act, joined(1))
                linear = linear.astype(jnp.bfloat16).astype(jnp.float32)
                gated = gated.astype(jnp.bfloat16).astype(jnp.float32)
                small = smalls[h]
                act = jax.nn.gelu(conv_rows(gated, small) + small[3:4], approximate=True)
                hidden.append((act * linear).astype(jnp.bfloat16))
            for j in range(n_fs):
                total = dot_nn(hidden[0], ffn_all[j, 0, 2]) + dot_nn(hidden[1], ffn_all[j, second, 2])
                total = total.astype(jnp.bfloat16).reshape(2, SEQ_LEN, width)
                pf[i, :, :, j * width : (j + 1) * width] = total
        for s in (1, 0):
            rs_core[i, s] = send(pf.at[i, s, theirs], rf.at[i, s], rs_s.at[0], rs_r.at[i, s], core)
            rs_core[i, s].start()

    def stage_core(i, s):
        wait(rs_core[i, s], f"rscore_{i}_{s}")
        for a in range(PARTS):
            at = pl.ds(a * part, part)
            ours = pl.ds(pl.multiple_of(c * share + a * part, part), part)
            total = pf[i, s, ours].astype(jnp.float32) + rf[i, s, at].astype(jnp.float32)
            sf[i, s, at] = total.astype(jnp.bfloat16)
            if s:
                rs_pair[i, a] = send(sf.at[i, s, at], rx.at[i, at], rs_s.at[1], rp_r.at[i, a], partner[i])
                rs_pair[i, a].start()

    rs_line = {}
    for i in range(1, 4):
        for a in range(PARTS):
            at = pl.ds(a * part, part)
            home = send(tf.at[i, at], rz.at[f, at], rs_s.at[2], rz_r.at[f, a], {"fs": places[i]})
            near_by = None
            if i > 1:
                near_by = send(tf.at[i, at], rq.at[i, at], rs_s.at[2], rq_r.at[i - 2, a], {"fs": places[1]})
            rs_line[i, a] = home, near_by
    owe(xs.at[:, 0], rs_s.at[0])
    owe(rz, rs_s.at[1])
    owe(rz.at[0:3], rs_s.at[2])

    def stage_pair(i, which=range(PARTS)):
        for a in which:
            at = pl.ds(a * part, part)
            wait(rs_pair[i, a], f"rspair_{i}_{a}")
            total = sf[i, 0, at].astype(jnp.float32) + rx[i, at].astype(jnp.float32)
            if i == 0:
                tf[i, at] = total.astype(jnp.bfloat16)
                continue
            home, near_by = rs_line[i, a]
            if near_by is None:
                tf[i, at] = total.astype(jnp.bfloat16)
                home.start()
                continue

            @pl.when(edge)
            def _():
                tf[i, at] = total.astype(jnp.bfloat16)
                near_by.start()

            @pl.when(inner)
            def _():
                wait(near_by, f"rq_{i}_{a}")
                tf[i, at] = (total + rq[i, at].astype(jnp.float32)).astype(jnp.bfloat16)
                home.start()

    def stage(i):
        stage_core(i, 1)
        stage_core(i, 0)

    half = SPREAD // 2
    spread(0)
    relay(EDGE[3], INNER[3])

    @pl.when(edge)
    def _():
        spread(1)
        pair_own()
        spread(2)
        pass_on(1)
        arrived(0)
        spread(3, range(half))

    @pl.when(inner)
    def _():
        spread(1)
        spread(2)
        spread(3)
        pair_own()
        pass_on(1)
        arrived(1)

    wait(own_side, "ffnown")
    wait(small_copy, "small")
    block(1)
    pl.when(edge)(functools.partial(spread, 3, range(half, SPREAD)))
    pass_on(2)
    stage(1)
    block(2)
    pass_on(3)
    stage_pair(1, (0,))
    stage(2)
    stage_pair(1, (1,))
    block(3)
    stage_pair(1, range(2, PARTS))
    pass_on(0)
    stage(3)
    pl.when(edge)(functools.partial(stage_pair, 2, (0, 1)))
    block(0)
    pl.when(edge)(functools.partial(stage_pair, 2, range(2, PARTS)))
    stage(0)
    pl.when(inner)(functools.partial(stage_pair, 2))
    stage_pair(3)
    stage_pair(0)

    def row_slot(who, a):
        return pl.ds(pl.multiple_of(who * share + a * part, part), part)

    fin = {}
    for a in range(PARTS):
        at = pl.ds(a * part, part)
        total = tf[0, at].astype(jnp.float32)
        for i in range(1, 3):
            ref = rz.at[places[i], at]
            landed(ref, rz_r.at[places[i], a], f"rz_{i}_{a}")
            total = total + rz[places[i], at].astype(jnp.float32)
        branch = total.astype(jnp.bfloat16).astype(jnp.float32)
        done = middle[at].astype(jnp.float32) + norm_rows(branch, gain_ffn_post[...][None])
        out[row_slot(t, a)] = done.astype(jnp.bfloat16)
        own = out.at[row_slot(t, a)]
        fin[a] = send(own, own, fin_s.at[0], fin_r.at[a], side)
        fin[a].start()
        send(own, own, fin_s.at[0], fin_r.at[PARTS], core).start()
    for a in range(PARTS):
        wait(fin[a], f"finside_{a}")
        far = out.at[row_slot(t_side, a)]
        send(far, far, fin_s.at[0], fin_r.at[PARTS + 1], core).start()
    for k in range(2):
        landed(rz.at[0], fin_r.at[PARTS + k], f"fincore_{k}")
    owe(rz.at[0:3], fin_s.at[0])
    settle_sends()


def split_plan(
    n_fs,
    stream,
    mix_pre_gain,
    w_outer_gate,
    w_inner_gate,
    w_value,
    mix_taps,
    w_mix_out,
    mix_post_gain,
    ffn_pre_gain,
    w_linear,
    w_gated,
    ffn_taps,
    ffn_bias,
    w_down,
    ffn_post_gain,
):
    rows, model = stream.shape
    width, conv_w = w_value.shape
    tiles = w_linear.shape[1] // (2 * PACK)
    few = tiles * 7 // 32 * PACK
    more = tiles * PACK - 2 * few
    cap = -(-more // (2 * PACK)) * PACK
    spans, at = [], 0
    for z in range(n_fs):
        both = (few, few) if z in (0, n_fs - 1) else (cap, more - cap)
        spans.append((at, *both))
        at += sum(both)
    share = rows // 4
    half = jnp.bfloat16
    vmem, dma = pltpu.VMEM, pltpu.SemaphoreType.DMA
    return pl.pallas_call(
        functools.partial(kernel, n_fs, conv_w, tuple(spans)),
        out_shape=pltpu.VMEM((rows, model), half),
        in_specs=[pl.BlockSpec(memory_space=pltpu.HBM)] * 15,
        out_specs=pl.BlockSpec(memory_space=vmem),
        scratch_shapes=[
            vmem((rows, model), half),
            vmem((model,), jnp.float32),
            vmem((model,), jnp.float32),
            vmem((model,), jnp.float32),
            vmem((model,), jnp.float32),
            vmem(mix_taps.shape, jnp.float32),
            vmem(w_down.shape, half),
            vmem(w_down.shape, half),
            vmem(w_down.shape, half),
            vmem(ffn_taps.shape, jnp.float32),
            vmem(ffn_bias.shape, jnp.float32),
            dma((12,)),
            vmem((n_fs, 2, 8, cap), jnp.float32),
            vmem((3, 8, cap), jnp.float32),
            vmem((n_fs, 3, cap, width), half),
            vmem((n_fs, 3, 3, cap, width), half),
            vmem((n_fs, 4 * conv_w, width), half),
            vmem((n_fs, rows, width), half),
            vmem((3, rows, conv_w), jnp.float32),
            vmem((2, SEQ_LEN, model), half),
            vmem((2, share, model), half),
            vmem((share, model), half),
            vmem((share, model), half),
            vmem((share, model), half),
            vmem((n_fs, 2, SEQ_LEN, model), half),
            vmem((n_fs, 2, SEQ_LEN, model), half),
            vmem((n_fs, 2, share, model), half),
            vmem((n_fs, 2, share, model), half),
            vmem((n_fs, share, model), half),
            vmem((n_fs, share, model), half),
            vmem((n_fs, share, model), half),
            vmem((n_fs, share, model), half),
            dma((1,)),
            dma((n_fs, CHUNKS)),
            dma((1,)),
            dma((3 * CHUNKS,)),
            dma((1,)),
            dma((3,)),
            dma((3,)),
            dma((n_fs, 3)),
            dma((1,)),
            dma((1,)),
            dma((3,)),
            dma((3,)),
            dma((2,)),
            dma((n_fs, SPREAD)),
            dma((3,)),
            dma((n_fs, SPREAD)),
            dma((2, n_fs)),
            dma((3,)),
            dma((n_fs, 2)),
            dma((n_fs, PARTS)),
            dma((n_fs, PARTS)),
            dma((2, PARTS)),
            dma((1,)),
            dma((PARTS + 2,)),
        ],
        compiler_params=pltpu.CompilerParams(
            collective_id=0, has_side_effects=True, vmem_limit_bytes=58 * 2**20
        ),
    )(
        stream,
        mix_pre_gain,
        mix_post_gain,
        ffn_pre_gain,
        ffn_post_gain,
        w_outer_gate.T,
        w_inner_gate.T,
        w_value.T,
        w_mix_out,
        mix_taps,
        w_linear.T,
        w_gated.T,
        w_down,
        ffn_taps,
        ffn_bias,
    )


def on_device(rep, n_fs, n_tp, *arrays):
    stream, w_value, w_linear = arrays[0], arrays[4], arrays[9]
    same = n_fs == n_tp == 2 * rep == 4
    whole = w_value.shape[0] % 128 == 0 and 2 * w_value.shape[1] % (CHUNKS * PACK) == 0
    even = w_linear.shape[1] % (2 * PACK) == 0 and stream.shape[0] == 2 * SEQ_LEN
    if same and whole and even:
        return split_plan(n_fs, *arrays)
    return gather_plan(*arrays)


def solution(mesh):
    in_specs = (
        P(("rep", "fs"), None),
        P(),
        P("fs", "tp"),
        P("fs", "tp"),
        P("fs", "tp"),
        P(None, "tp"),
        P("tp", "fs"),
        P(),
        P(),
        P("fs", "tp"),
        P("fs", "tp"),
        P(None, "tp"),
        P("tp"),
        P("tp", "fs"),
        P(),
    )
    out_specs = P(("rep", "fs"), None)
    sizes = mesh.shape
    body = functools.partial(on_device, sizes["rep"], sizes["fs"], sizes["tp"])
    return jax.shard_map(
        body, mesh=mesh, in_specs=in_specs, out_specs=out_specs, check_vma=False
    )
```

```python
import contextlib
import functools

import jax
import jax.numpy as jnp
from jax import lax
from jax.experimental import pallas as pl
from jax.experimental.pallas import tpu as pltpu
from jax.sharding import PartitionSpec as P

SEQ_LEN = 128
PACK = 16
CHUNKS = 4
SPREAD = 2
PARTS = 4
JOIN = 2
FIRST = (0, 1)
EDGE = (
    (),
    (),
    ((3, 0), (3, 1), (3, 2), (1, 0)),
    ((1, 1), (1, 2), (2, 0), (2, 1), (2, 2)),
)
INNER = (
    ((1, 0), (1, 1), (1, 2)),
    ((3, 0), (3, 1)),
    ((3, 2), (2, 0), (2, 1)),
    ((2, 2),),
)
SIDEWAYS = ((True, False, False, True), (True, True, True, False))
TRACE = False


EPS = 1e-06


def norm_scale(values, gain):
    return values * lax.rsqrt(jnp.mean(values * values, axis=-1, keepdims=True) + EPS) * gain


def conv_three(values, taps):
    height, breadth = values.shape
    grouped = values.reshape(height // SEQ_LEN, SEQ_LEN, breadth)
    padded = jnp.pad(grouped, ((0, 0), (1, 1), (0, 0)))
    mixed = taps[0] * padded[:, :-2] + taps[1] * padded[:, 1:-1] + taps[2] * padded[:, 2:]
    return mixed.reshape(height, breadth)


def settle(partial_value, resid, post_gain):
    branch = lax.psum(partial_value.astype(jnp.bfloat16), "tp")
    return (resid + norm_scale(branch.astype(jnp.float32), post_gain)).astype(jnp.bfloat16)


def gather_plan(
    stream,
    mix_pre_gain,
    w_outer_gate,
    w_inner_gate,
    w_value,
    mix_taps,
    w_mix_out,
    mix_post_gain,
    ffn_pre_gain,
    w_linear,
    w_gated,
    ffn_taps,
    ffn_bias,
    w_down,
    ffn_post_gain,
):
    resid = stream.astype(jnp.float32)
    normed = norm_scale(resid, mix_pre_gain).astype(jnp.bfloat16)
    full_outer, full_inner, full_value = (
        lax.all_gather(w_outer_gate, "fs", axis=0, tiled=True),
        lax.all_gather(w_inner_gate, "fs", axis=0, tiled=True),
        lax.all_gather(w_value, "fs", axis=0, tiled=True),
    )
    outer = jnp.dot(normed, full_outer, preferred_element_type=jnp.float32)
    inner = jnp.dot(normed, full_inner, preferred_element_type=jnp.float32)
    value = jnp.dot(normed, full_value, preferred_element_type=jnp.float32)
    outer = outer.astype(jnp.bfloat16)
    inner = inner.astype(jnp.bfloat16)
    value = value.astype(jnp.bfloat16)
    product = inner.astype(jnp.float32) * value.astype(jnp.float32)
    mixed = (outer.astype(jnp.float32) * conv_three(product, mix_taps)).astype(jnp.bfloat16)
    full_mix_out = lax.all_gather(w_mix_out, "fs", axis=1, tiled=True)
    partial_value = jnp.dot(mixed, full_mix_out, preferred_element_type=jnp.float32)
    middle = settle(partial_value, resid, mix_post_gain)
    middle_f = middle.astype(jnp.float32)
    normed_two = norm_scale(middle_f, ffn_pre_gain).astype(jnp.bfloat16)
    full_linear, full_gated = (
        lax.all_gather(w_linear, "fs", axis=0, tiled=True),
        lax.all_gather(w_gated, "fs", axis=0, tiled=True),
    )
    linear = jnp.dot(normed_two, full_linear, preferred_element_type=jnp.float32)
    gated = jnp.dot(normed_two, full_gated, preferred_element_type=jnp.float32)
    linear = linear.astype(jnp.bfloat16)
    gated = gated.astype(jnp.bfloat16)
    activated = jax.nn.gelu(
        conv_three(gated.astype(jnp.float32), ffn_taps) + ffn_bias, approximate=True
    )
    hidden = (activated * linear.astype(jnp.float32)).astype(jnp.bfloat16)
    full_down = lax.all_gather(w_down, "fs", axis=1, tiled=True)
    partial_two = jnp.dot(hidden, full_down, preferred_element_type=jnp.float32)
    return settle(partial_two, middle_f, ffn_post_gain)


def dot_nt(left, right):
    return lax.dot_general(left, right, (((1,), (1,)), ((), ())), preferred_element_type=jnp.float32)


def dot_nn(left, right):
    return jnp.dot(left, right, preferred_element_type=jnp.float32)


def conv_rows(values, taps):
    height = values.shape[0]
    row = lax.broadcasted_iota(jnp.int32, values.shape, 0) % SEQ_LEN
    before = jnp.where(row == 0, 0.0, pltpu.roll(values, 1, 0))
    after = jnp.where(row == SEQ_LEN - 1, 0.0, pltpu.roll(values, height - 1, 0))
    return taps[0:1] * before + taps[1:2] * values + taps[2:3] * after


def norm_rows(values, gain):
    scale = lax.rsqrt(jnp.mean(values * values, axis=-1, keepdims=True) + EPS)
    return values * scale * gain


def scope(name):
    return jax.named_scope(name) if TRACE else contextlib.nullcontext()


def kernel(n_fs, conv_w, spans, *refs):
    sources, out, scratch = refs[:15], refs[15], refs[16:]
    (
        stream,
        gain_mix_pre,
        gain_mix_post,
        gain_ffn_pre,
        gain_ffn_post,
        mix_taps,
        w_linear,
        w_gated,
        w_down,
        ffn_taps,
        ffn_bias,
        load_s,
        small_all,
        smalls,
        small_pair,
        ffn_w,
        ffn_all,
        mix_all,
        normed,
        acc,
        pm,
        rm,
        sm,
        rxm,
        middle,
        xs,
        pf,
        rf,
        sf,
        rx,
        tf,
        rz,
        rq,
        mz_s,
        mz_r,
        my_s,
        my_r,
        mr_s,
        mr_r,
        fz_s,
        fz_r,
        fy_s,
        fy_r,
        fx_s,
        fx_r,
        az_s,
        az_r,
        ap_s,
        ap_r,
        ac_r,
        rs_s,
        rs_r,
        rp_r,
        rz_r,
        rq_r,
        fin_s,
        fin_r,
    ) = scratch
    r, f, t = lax.axis_index("rep"), lax.axis_index("fs"), lax.axis_index("tp")
    x, c = t // 2, t % 2
    t_core, t_side = 2 * x + 1 - c, 2 * (1 - x) + c
    core, side, other = {"tp": t_core}, {"tp": t_side}, {"rep": 1 - r}
    rows, width = stream.shape[0], ffn_w.shape[3]
    cap, few = ffn_w.shape[2], spans[0][1]
    sizes = (few, cap)
    share = rows // 4
    mine = pl.ds(pl.multiple_of(c * share, share), share)
    theirs = pl.ds(pl.multiple_of((1 - c) * share, share), share)

    near = f < n_fs // 2
    mirror = lambda v: jnp.where(near, v, n_fs - 1 - v)
    inner = jnp.where(near, f, n_fs - 1 - f) == 1
    edge = jnp.logical_not(inner)
    order = [mirror(jnp.where(inner, 0, 1)), mirror(2), mirror(3)]
    goals = [mirror(jnp.where(inner, 2, 1)), mirror(jnp.where(inner, 3, 2)), mirror(jnp.where(inner, 0, 3))]
    upward, downward = mirror(jnp.where(inner, 2, 1)), mirror(0)
    places = [f] + order

    def send(src, dst, ss, rs, where):
        return pltpu.make_async_remote_copy(
            src_ref=src,
            dst_ref=dst,
            send_sem=ss,
            recv_sem=rs,
            device_id=where,
            device_id_type=pl.DeviceIdType.MESH,
        )

    owed = []

    def owe(ref, sem, when=None):
        owed.append((send(ref, ref, sem, sem, core), when))

    def settle_sends():
        for copy, when in owed:
            if when is None:
                copy.wait_send()
            else:
                pl.when(when)(copy.wait_send)

    def begin(copy, when=None):
        if when is None:
            copy.start()
        else:
            pl.when(when)(copy.start)

    def landed(ref, sem, name):
        wait(send(ref, ref, sem, sem, core), name)

    def wait(copy, name):
        with scope(name):
            copy.wait_recv()

    barrier = pltpu.get_barrier_semaphore()
    peers = [core, side, other] + [{"fs": (f + k) % n_fs} for k in (1, 2, 3)]
    for peer in peers:
        pl.semaphore_signal(barrier, inc=1, device_id=peer, device_id_type=pl.DeviceIdType.MESH)
    targets = [mix_all.at[f, p * conv_w : (p + 1) * conv_w] for p in range(4)]
    targets += [stream, gain_mix_pre, w_linear, w_gated, w_down, ffn_taps, ffn_bias]
    targets += [gain_mix_post, gain_ffn_pre, gain_ffn_post, mix_taps]
    places_in = (5, 6, 7, 8, 0, 1, 10, 11, 12, 13, 14, 2, 3, 4, 9)
    loads = [
        pltpu.make_async_copy(sources[i], ref, load_s.at[max(k - 3, 0)])
        for k, (i, ref) in enumerate(zip(places_in, targets))
    ]
    for load in loads:
        load.start()
    pltpu.make_async_copy(mix_all.at[f], mix_all.at[f], load_s.at[0]).wait()
    with scope("barrier"):
        pl.semaphore_wait(barrier, len(peers))

    mix_half = mix_all.shape[1] // 2
    mix_cut = mix_half // CHUNKS

    def mix_copy(b, h, to):
        at = pl.ds(pl.multiple_of(r * mix_half + h * mix_cut, PACK), mix_cut)
        ref = mix_all.at[b, at]
        return send(ref, ref, mz_s.at[0], mz_r.at[b, h], {"fs": to})

    for h in range(CHUNKS):
        begin(mix_copy(f, h, upward))
        begin(mix_copy(f, h, downward), inner)
    owe(mix_all.at[0, 0:mix_half], mz_s.at[0], edge)
    owe(mix_all.at[0:n_fs, 0 : mix_half * 5 // n_fs], mz_s.at[0], inner)

    for load in loads[6:]:
        load.wait()

    pieces = (w_linear, w_gated, w_down)

    def keep(ref, at, size, piece):
        ref[0:size] = piece[at : at + size]
        if size < cap:
            ref[size:cap] = jnp.zeros((cap - size, width), ffn_w.dtype)

    for half in range(2):

        @pl.when(r == half)
        def _():
            for j, (at, *both) in enumerate(spans):
                for p, piece in enumerate(pieces):
                    keep(ffn_w.at[j, p], at + half * both[0], both[half], piece)

    narrow = ((cap, cap, few), (cap, few, few))

    def ffn_send(kind, i):
        for p in range(3):
            at = slice(0, narrow[kind][i])
            src, dst = ffn_w.at[goals[i], p, at], ffn_all.at[f, 0, p, at]
            yield send(src, dst, fz_s.at[i], fz_r.at[f, p], {"fs": goals[i]})

    kinds = (edge, inner)
    ffn_out = [[list(ffn_send(kind, i)) for i in range(3)] for kind in range(2)]
    for kind in range(2):
        for i in range(3):
            owe(ffn_w.at[0, :, 0 : narrow[kind][i]], fz_s.at[i], kinds[kind])

    def ffn_start(kind, *which):
        for i in which:
            for copy in ffn_out[kind][i]:
                copy.start()

    pl.when(edge)(functools.partial(ffn_start, 0, 0, 1, 2))

    own_side = send(ffn_w.at[f], ffn_all.at[f, 2], fx_s.at[0], fx_r.at[0], side)
    own_side.start()
    owe(ffn_w.at[f], fx_s.at[0])
    for p in range(3):
        ffn_all[f, 0, p] = ffn_w[f, p]
    for j, (at, *both) in enumerate(spans):
        for half in range(2):

            @pl.when((f == j) & (r == half))
            def _():
                for p, piece in enumerate(pieces):
                    keep(ffn_all.at[j, 1, p], at + (1 - half) * both[0], both[1 - half], piece)

    @pl.when(edge)
    def _():
        for i in range(1, 4):
            ffn_all[places[i], :, :, few:cap] = jnp.zeros((3, 3, cap - few, width), ffn_w.dtype)

    small_all[...] = jnp.zeros(small_all.shape, jnp.float32)
    for j, (first, *both) in enumerate(spans):
        for half, size in enumerate(both):
            at = first + half * both[0]
            small_all[j, half, 0:3, 0:size] = ffn_taps[:, at : at + size]
            small_all[j, half, 3:4, 0:size] = ffn_bias[at : at + size][None]
    smalls[0] = small_all[f, r]
    smalls[1] = small_all[f, 1 - r]
    small_copy = send(smalls.at[0], smalls.at[2], fx_s.at[1], fx_r.at[1], side)
    small_copy.start()
    owe(smalls.at[0], fx_s.at[1])

    for load in loads[4:6]:
        load.wait()
    step_rows = 32

    @pl.loop(0, rows // step_rows)
    def _(i):
        at = pl.ds(pl.multiple_of(i * step_rows, step_rows), step_rows)
        value = norm_rows(stream[at].astype(jnp.float32), gain_mix_pre[...][None]).astype(jnp.bfloat16)
        for j in range(n_fs):
            normed[j, at] = value[:, j * width : (j + 1) * width]

    def project(z, first=False):
        for p in range(3):
            term = dot_nt(normed[z], mix_all[z, p * conv_w : (p + 1) * conv_w])
            acc[p] = term if first else acc[p] + term

    project(f, True)

    flows = [(i, h) for i in range(3) for h in range(CHUNKS)]
    turns = [(i, h) for h in range(CHUNKS) for i in range(2)] + [(2, h) for h in range(CHUNKS)]
    my = []
    for e in range(3 * CHUNKS):
        (i_edge, h_edge), (i_inner, h_inner) = flows[e], turns[e]
        b = jnp.where(inner, order[i_inner], order[i_edge])
        h = jnp.where(inner, h_inner, h_edge)
        onward = downward if i_inner > 0 else upward
        copy = mix_copy(b, h, onward)
        wait(copy, f"mixz_{e}")
        begin(copy, inner)
        at = pl.ds(pl.multiple_of(r * mix_half + h * mix_cut, PACK), mix_cut)
        ref = mix_all.at[b, at]
        my.append(send(ref, ref, my_s.at[0], my_r.at[e], other))
        my[e].start()
        if e == 2 * CHUNKS - 2:
            pl.when(inner)(functools.partial(ffn_start, 1, *FIRST))
    owe(mix_all.at[0:3, 0:mix_half], my_s.at[0])
    pl.when(inner)(functools.partial(ffn_start, 1, 2))

    def hop(kind, i, p, piece, ss, rs, to):
        src = ffn_all.at[places[i], 0, p, 0 : sizes[kind]]
        dst = ffn_all.at[places[i], piece, p, 0 : sizes[kind]]
        return send(src, dst, ss, rs, to)

    trips = [(i, p) for i in range(1, 4) for p in range(3)]
    fy = [{(i, p): hop(kind, i, p, 1, fy_s.at[0], fy_r.at[0], other) for i, p in trips} for kind in range(2)]
    fx = [{(i, p): hop(kind, i, p, 2, fx_s.at[2], fx_r.at[2], side) for i, p in trips} for kind in range(2)]
    all_trips = [ffn_all.at[0:3, 0, :, 0 : sizes[kind]] for kind in range(2)]
    for kind in range(2):
        owe(all_trips[kind], fy_s.at[0], kinds[kind])
        owe(all_trips[kind], fx_s.at[2], kinds[kind])

    def forward(kind, *which):
        for i, p in which:
            src = ffn_all.at[places[i], 0, p, 0 : sizes[kind]]
            wait(send(src, src, fz_s.at[i - 1], fz_r.at[places[i], p], other), f"ffnz_{i}_{p}")
            fy[kind][i, p].start()
            fx[kind][i, p].start()

    def relay(edge_list, inner_list):
        for kind, which in enumerate((edge_list, inner_list)):
            if which:
                pl.when(kinds[kind])(functools.partial(forward, kind, *which))

    def arrived(kind):
        landed(all_trips[kind], fy_r.at[0], "ffny")
        landed(all_trips[kind], fx_r.at[2], "ffnx")

    relay(EDGE[0], INNER[0])
    for e in range(3 * CHUNKS):
        if e == 2 * CHUNKS:
            relay(EDGE[1], INNER[1])
        wait(my[e], f"mixy_{e}")
        if e == 2 * CHUNKS - 1:
            project(order[0])
            project(order[1])
    project(order[2])

    mix_core = []
    for k, q in enumerate((1 - x, x)):
        here = pl.ds(pl.multiple_of(q * SEQ_LEN, SEQ_LEN), SEQ_LEN)
        parts = [acc[p, here].astype(jnp.bfloat16).astype(jnp.float32) for p in range(3)]
        mixed = (parts[0] * conv_rows(parts[1] * parts[2], mix_taps)).astype(jnp.bfloat16)
        for j in range(n_fs):
            pm[k, :, j * width : (j + 1) * width] = dot_nn(
                mixed, mix_all[j, 3 * conv_w : 4 * conv_w]
            ).astype(jnp.bfloat16)
        mix_core.append(send(pm.at[k, theirs], rm.at[k], mr_s.at[0], mr_r.at[k], core))
        mix_core[k].start()

    def mix_sum(k):
        wait(mix_core[k], f"mixcore_{k}")
        return (pm[k, mine].astype(jnp.float32) + rm[k].astype(jnp.float32)).astype(jnp.bfloat16)

    sm[...] = mix_sum(0)
    mix_side = send(sm, rxm, mr_s.at[0], mr_r.at[2], side)
    mix_side.start()
    owe(rz.at[0:3], mr_s.at[0])

    kept = mix_sum(1)
    relay(EDGE[2], INNER[2])
    wait(mix_side, "mixside")
    branch = (kept.astype(jnp.float32) + rxm[...].astype(jnp.float32)).astype(jnp.bfloat16)
    slot = pl.ds(pl.multiple_of(t * share, share), share)
    mid = stream[slot].astype(jnp.float32) + norm_rows(branch.astype(jnp.float32), gain_mix_post[...][None])
    mid = mid.astype(jnp.bfloat16)
    middle[...] = mid
    xs[f, 0, mine] = norm_rows(mid.astype(jnp.float32), gain_ffn_pre[...][None]).astype(jnp.bfloat16)

    sideways = [jnp.where(edge, a, b) for a, b in zip(*SIDEWAYS)]
    partner = [{"rep": jnp.where(a, r, 1 - r), "tp": jnp.where(a, t_side, t)} for a in sideways]
    cut = share // SPREAD

    def piece_of(z, s, a):
        return xs.at[z, s, pl.ds(pl.multiple_of(c * share + a * cut, cut), cut)]

    ag_core, ag_pair, ag_pass = {}, {}, {}

    slab = pl.ds(pl.multiple_of(c * share, share), share)
    slab_core = pl.ds(pl.multiple_of((1 - c) * share, share), share)
    for i in range(4):
        for a in range(SPREAD):
            src, far = piece_of(places[i], 0, a), piece_of(places[i], 1, a)
            ag_pair[i, a] = send(src, far, ap_s.at[0], ap_r.at[i, a], partner[i])
            ag_core[i, a] = send(src, src, ap_s.at[1], ac_r.at[0, i], core)
            ag_pass[i, a] = send(far, far, ap_s.at[2], ac_r.at[1, i], core)
    for k in range(3):
        owe(rz, ap_s.at[k])
    owe(rz.at[0], az_s.at[0])
    owe(rz, az_s.at[1], inner)

    def pair_own():
        for a in range(SPREAD):
            ag_pair[0, a].start()

    def spread(i, which=range(SPREAD)):
        for a in which:
            src = piece_of(places[i], 0, a)
            if i == 0:
                send(src, src, az_s.at[0], az_r.at[f, a], {"fs": upward}).start()
                begin(send(src, src, az_s.at[1], az_r.at[f, a], {"fs": downward}), inner)
            else:
                copy = send(src, src, az_s.at[1], az_r.at[places[i], a], {"fs": downward if i > 1 else upward})
                wait(copy, f"agz_{i}_{a}")
                begin(copy, inner)
                ag_pair[i, a].start()
            ag_core[i, a].start()

    def pass_on(i):
        for a in range(SPREAD):
            wait(ag_pair[i, a], f"agpair_{i}_{a}")
            ag_pass[i, a].start()

    rs_core, rs_pair = {}, {}
    part = share // PARTS

    def activate(linear, gated, small):
        linear = linear.astype(jnp.bfloat16).astype(jnp.float32)
        gated = gated.astype(jnp.bfloat16).astype(jnp.float32)
        act = jax.nn.gelu(conv_rows(gated, small) + small[3:4], approximate=True)
        return (act * linear).astype(jnp.bfloat16)

    def raise_up(z, weights):
        linear, gated = 0.0, 0.0
        for j in range(0, n_fs, JOIN):
            act = xs[z, :, :, j * width : (j + JOIN) * width].reshape(2 * SEQ_LEN, JOIN * width)
            joined = lambda p: jnp.concatenate([weights(j + k, p) for k in range(JOIN)], axis=1)
            linear = linear + dot_nt(act, joined(0))
            gated = gated + dot_nt(act, joined(1))
        return linear, gated

    def keep_partial(i, j, total):
        pf[i, :, :, j * width : (j + 1) * width] = total.astype(jnp.bfloat16).reshape(2, SEQ_LEN, width)

    def block_edge(i):
        second = 1 if SIDEWAYS[0][i] else 2
        both = lambda j, p: jnp.concatenate([ffn_all[j, h, p, 0:few] for h in (0, second)], axis=0)
        hidden = activate(*raise_up(places[i], both), small_pair[second - 1])
        for j in range(n_fs):
            keep_partial(i, j, dot_nn(hidden, both(j, 2)))

    def block_inner(i):
        second = 1 if SIDEWAYS[1][i] else 2
        hidden = [
            activate(*raise_up(places[i], lambda j, p: ffn_all[j, h, p]), smalls[h]) for h in (0, second)
        ]
        for j in range(n_fs):
            total = dot_nn(hidden[0], ffn_all[j, 0, 2]) + dot_nn(hidden[1], ffn_all[j, second, 2])
            keep_partial(i, j, total)

    def block(i):
        for s in range(2):
            landed(xs.at[places[i], s, slab_core], ac_r.at[s, i], f"agcore_{i}_{s}")
        for kind in range(2):
            pl.when(kinds[kind])(functools.partial((block_edge, block_inner)[kind], i))
        for s in (1, 0):
            rs_core[i, s] = send(pf.at[i, s, theirs], rf.at[i, s], rs_s.at[0], rs_r.at[i, s], core)
            rs_core[i, s].start()

    def stage_core(i, s):
        wait(rs_core[i, s], f"rscore_{i}_{s}")
        for a in range(PARTS):
            at = pl.ds(a * part, part)
            ours = pl.ds(pl.multiple_of(c * share + a * part, part), part)
            total = pf[i, s, ours].astype(jnp.float32) + rf[i, s, at].astype(jnp.float32)
            sf[i, s, at] = total.astype(jnp.bfloat16)
            if s:
                rs_pair[i, a] = send(sf.at[i, s, at], rx.at[i, at], rs_s.at[1], rp_r.at[i, a], partner[i])
                rs_pair[i, a].start()

    rs_line = {}
    for i in range(1, 4):
        for a in range(PARTS):
            at = pl.ds(a * part, part)
            home = send(tf.at[i, at], rz.at[f, at], rs_s.at[2], rz_r.at[f, a], {"fs": places[i]})
            near_by = None
            if i > 1:
                near_by = send(tf.at[i, at], rq.at[i, at], rs_s.at[2], rq_r.at[i - 2, a], {"fs": places[1]})
            rs_line[i, a] = home, near_by
    owe(xs.at[:, 0], rs_s.at[0])
    owe(rz, rs_s.at[1])
    owe(rz.at[0:3], rs_s.at[2])

    def stage_pair(i, which=range(PARTS)):
        for a in which:
            at = pl.ds(a * part, part)
            wait(rs_pair[i, a], f"rspair_{i}_{a}")
            total = sf[i, 0, at].astype(jnp.float32) + rx[i, at].astype(jnp.float32)
            if i == 0:
                tf[i, at] = total.astype(jnp.bfloat16)
                continue
            home, near_by = rs_line[i, a]
            if near_by is None:
                tf[i, at] = total.astype(jnp.bfloat16)
                home.start()
                continue

            @pl.when(edge)
            def _():
                tf[i, at] = total.astype(jnp.bfloat16)
                near_by.start()

            @pl.when(inner)
            def _():
                wait(near_by, f"rq_{i}_{a}")
                tf[i, at] = (total + rq[i, at].astype(jnp.float32)).astype(jnp.bfloat16)
                home.start()

    def stage(i):
        stage_core(i, 1)
        stage_core(i, 0)

    spread(0)
    relay(EDGE[3], INNER[3])

    @pl.when(edge)
    def _():
        spread(1)
        pair_own()
        spread(2)
        pass_on(1)
        arrived(0)

    @pl.when(inner)
    def _():
        spread(1)
        spread(2)
        spread(3)
        pair_own()
        pass_on(1)
        arrived(1)

    wait(own_side, "ffnown")
    wait(small_copy, "small")
    for k in range(2):
        small_pair[k, :, 0:few] = smalls[0, :, 0:few]
        small_pair[k, :, few : 2 * few] = smalls[k + 1, :, 0:few]
    block(1)
    pl.when(edge)(functools.partial(spread, 3))
    pass_on(2)
    stage(1)
    block(2)
    pass_on(3)
    stage_pair(1, (0,))
    stage(2)
    stage_pair(1, (1,))
    block(3)
    stage_pair(1, range(2, PARTS))
    pass_on(0)
    stage(3)
    pl.when(edge)(functools.partial(stage_pair, 2, (0, 1)))
    block(0)
    pl.when(edge)(functools.partial(stage_pair, 2, range(2, PARTS)))
    stage(0)
    pl.when(inner)(functools.partial(stage_pair, 2))
    stage_pair(3)
    stage_pair(0)

    def row_slot(who, a):
        return pl.ds(pl.multiple_of(who * share + a * part, part), part)

    fin = {}
    for a in range(PARTS):
        at = pl.ds(a * part, part)
        total = tf[0, at].astype(jnp.float32)
        for i in range(1, 3):
            ref = rz.at[places[i], at]
            landed(ref, rz_r.at[places[i], a], f"rz_{i}_{a}")
            total = total + rz[places[i], at].astype(jnp.float32)
        branch = total.astype(jnp.bfloat16).astype(jnp.float32)
        done = middle[at].astype(jnp.float32) + norm_rows(branch, gain_ffn_post[...][None])
        out[row_slot(t, a)] = done.astype(jnp.bfloat16)
        own = out.at[row_slot(t, a)]
        fin[a] = send(own, own, fin_s.at[0], fin_r.at[a], side)
        fin[a].start()
        send(own, own, fin_s.at[0], fin_r.at[PARTS], core).start()
    for a in range(PARTS):
        wait(fin[a], f"finside_{a}")
        far = out.at[row_slot(t_side, a)]
        send(far, far, fin_s.at[0], fin_r.at[PARTS + 1], core).start()
    for k in range(2):
        landed(rz.at[0], fin_r.at[PARTS + k], f"fincore_{k}")
    owe(rz.at[0:3], fin_s.at[0])
    settle_sends()


def split_plan(
    n_fs,
    stream,
    mix_pre_gain,
    w_outer_gate,
    w_inner_gate,
    w_value,
    mix_taps,
    w_mix_out,
    mix_post_gain,
    ffn_pre_gain,
    w_linear,
    w_gated,
    ffn_taps,
    ffn_bias,
    w_down,
    ffn_post_gain,
):
    rows, model = stream.shape
    width, conv_w = w_value.shape
    tiles = w_linear.shape[1] // (2 * PACK)
    few = tiles * 7 // 32 * PACK
    more = tiles * PACK - 2 * few
    cap = -(-more // (2 * PACK)) * PACK
    spans, at = [], 0
    for z in range(n_fs):
        both = (few, few) if z in (0, n_fs - 1) else (cap, more - cap)
        spans.append((at, *both))
        at += sum(both)
    share = rows // 4
    half = jnp.bfloat16
    vmem, dma = pltpu.VMEM, pltpu.SemaphoreType.DMA
    return pl.pallas_call(
        functools.partial(kernel, n_fs, conv_w, tuple(spans)),
        out_shape=pltpu.VMEM((rows, model), half),
        in_specs=[pl.BlockSpec(memory_space=pltpu.HBM)] * 15,
        out_specs=pl.BlockSpec(memory_space=vmem),
        scratch_shapes=[
            vmem((rows, model), half),
            vmem((model,), jnp.float32),
            vmem((model,), jnp.float32),
            vmem((model,), jnp.float32),
            vmem((model,), jnp.float32),
            vmem(mix_taps.shape, jnp.float32),
            vmem(w_down.shape, half),
            vmem(w_down.shape, half),
            vmem(w_down.shape, half),
            vmem(ffn_taps.shape, jnp.float32),
            vmem(ffn_bias.shape, jnp.float32),
            dma((12,)),
            vmem((n_fs, 2, 8, cap), jnp.float32),
            vmem((3, 8, cap), jnp.float32),
            vmem((2, 8, 2 * few), jnp.float32),
            vmem((n_fs, 3, cap, width), half),
            vmem((n_fs, 3, 3, cap, width), half),
            vmem((n_fs, 4 * conv_w, width), half),
            vmem((n_fs, rows, width), half),
            vmem((3, rows, conv_w), jnp.float32),
            vmem((2, SEQ_LEN, model), half),
            vmem((2, share, model), half),
            vmem((share, model), half),
            vmem((share, model), half),
            vmem((share, model), half),
            vmem((n_fs, 2, SEQ_LEN, model), half),
            vmem((n_fs, 2, SEQ_LEN, model), half),
            vmem((n_fs, 2, share, model), half),
            vmem((n_fs, 2, share, model), half),
            vmem((n_fs, share, model), half),
            vmem((n_fs, share, model), half),
            vmem((n_fs, share, model), half),
            vmem((n_fs, share, model), half),
            dma((1,)),
            dma((n_fs, CHUNKS)),
            dma((1,)),
            dma((3 * CHUNKS,)),
            dma((1,)),
            dma((3,)),
            dma((3,)),
            dma((n_fs, 3)),
            dma((1,)),
            dma((1,)),
            dma((3,)),
            dma((3,)),
            dma((2,)),
            dma((n_fs, SPREAD)),
            dma((3,)),
            dma((n_fs, SPREAD)),
            dma((2, n_fs)),
            dma((3,)),
            dma((n_fs, 2)),
            dma((n_fs, PARTS)),
            dma((n_fs, PARTS)),
            dma((2, PARTS)),
            dma((1,)),
            dma((PARTS + 2,)),
        ],
        compiler_params=pltpu.CompilerParams(
            collective_id=0, has_side_effects=True, vmem_limit_bytes=58 * 2**20
        ),
    )(
        stream,
        mix_pre_gain,
        mix_post_gain,
        ffn_pre_gain,
        ffn_post_gain,
        w_outer_gate.T,
        w_inner_gate.T,
        w_value.T,
        w_mix_out,
        mix_taps,
        w_linear.T,
        w_gated.T,
        w_down,
        ffn_taps,
        ffn_bias,
    )


def on_device(rep, n_fs, n_tp, *arrays):
    stream, w_value, w_linear = arrays[0], arrays[4], arrays[9]
    same = n_fs == n_tp == 2 * rep == 4
    whole = w_value.shape[0] % 128 == 0 and 2 * w_value.shape[1] % (CHUNKS * PACK) == 0
    even = w_linear.shape[1] % (2 * PACK) == 0 and stream.shape[0] == 2 * SEQ_LEN
    if same and whole and even:
        return split_plan(n_fs, *arrays)
    return gather_plan(*arrays)


def solution(mesh):
    in_specs = (
        P(("rep", "fs"), None),
        P(),
        P("fs", "tp"),
        P("fs", "tp"),
        P("fs", "tp"),
        P(None, "tp"),
        P("tp", "fs"),
        P(),
        P(),
        P("fs", "tp"),
        P("fs", "tp"),
        P(None, "tp"),
        P("tp"),
        P("tp", "fs"),
        P(),
    )
    out_specs = P(("rep", "fs"), None)
    sizes = mesh.shape
    body = functools.partial(on_device, sizes["rep"], sizes["fs"], sizes["tp"])
    return jax.shard_map(
        body, mesh=mesh, in_specs=in_specs, out_specs=out_specs, check_vma=False
    )
```

```python
import contextlib
import functools

import jax
import jax.numpy as jnp
from jax import lax
from jax.experimental import pallas as pl
from jax.experimental.pallas import tpu as pltpu
from jax.sharding import PartitionSpec as P

SEQ_LEN = 128
PACK = 16
CHUNKS = 4
SPREAD = 2
PARTS = 4
JOIN = 2
FIRST = (0, 1)
EDGE = (
    (),
    (),
    ((3, 0), (3, 1), (3, 2), (1, 0)),
    ((1, 1), (1, 2), (2, 0), (2, 1), (2, 2)),
)
INNER = (
    ((1, 0), (1, 1), (1, 2)),
    ((3, 0), (3, 1)),
    ((3, 2), (2, 0), (2, 1)),
    ((2, 2),),
)
SIDEWAYS = ((True, False, False, True), (True, True, True, False))
TRACE = False


EPS = 1e-06


def norm_scale(values, gain):
    return values * lax.rsqrt(jnp.mean(values * values, axis=-1, keepdims=True) + EPS) * gain


def conv_three(values, taps):
    height, breadth = values.shape
    grouped = values.reshape(height // SEQ_LEN, SEQ_LEN, breadth)
    padded = jnp.pad(grouped, ((0, 0), (1, 1), (0, 0)))
    mixed = taps[0] * padded[:, :-2] + taps[1] * padded[:, 1:-1] + taps[2] * padded[:, 2:]
    return mixed.reshape(height, breadth)


def settle(partial_value, resid, post_gain):
    branch = lax.psum(partial_value.astype(jnp.bfloat16), "tp")
    return (resid + norm_scale(branch.astype(jnp.float32), post_gain)).astype(jnp.bfloat16)


def gather_plan(
    stream,
    mix_pre_gain,
    w_outer_gate,
    w_inner_gate,
    w_value,
    mix_taps,
    w_mix_out,
    mix_post_gain,
    ffn_pre_gain,
    w_linear,
    w_gated,
    ffn_taps,
    ffn_bias,
    w_down,
    ffn_post_gain,
):
    resid = stream.astype(jnp.float32)
    normed = norm_scale(resid, mix_pre_gain).astype(jnp.bfloat16)
    full_outer, full_inner, full_value = (
        lax.all_gather(w_outer_gate, "fs", axis=0, tiled=True),
        lax.all_gather(w_inner_gate, "fs", axis=0, tiled=True),
        lax.all_gather(w_value, "fs", axis=0, tiled=True),
    )
    outer = jnp.dot(normed, full_outer, preferred_element_type=jnp.float32)
    inner = jnp.dot(normed, full_inner, preferred_element_type=jnp.float32)
    value = jnp.dot(normed, full_value, preferred_element_type=jnp.float32)
    outer = outer.astype(jnp.bfloat16)
    inner = inner.astype(jnp.bfloat16)
    value = value.astype(jnp.bfloat16)
    product = inner.astype(jnp.float32) * value.astype(jnp.float32)
    mixed = (outer.astype(jnp.float32) * conv_three(product, mix_taps)).astype(jnp.bfloat16)
    full_mix_out = lax.all_gather(w_mix_out, "fs", axis=1, tiled=True)
    partial_value = jnp.dot(mixed, full_mix_out, preferred_element_type=jnp.float32)
    middle = settle(partial_value, resid, mix_post_gain)
    middle_f = middle.astype(jnp.float32)
    normed_two = norm_scale(middle_f, ffn_pre_gain).astype(jnp.bfloat16)
    full_linear, full_gated = (
        lax.all_gather(w_linear, "fs", axis=0, tiled=True),
        lax.all_gather(w_gated, "fs", axis=0, tiled=True),
    )
    linear = jnp.dot(normed_two, full_linear, preferred_element_type=jnp.float32)
    gated = jnp.dot(normed_two, full_gated, preferred_element_type=jnp.float32)
    linear = linear.astype(jnp.bfloat16)
    gated = gated.astype(jnp.bfloat16)
    activated = jax.nn.gelu(
        conv_three(gated.astype(jnp.float32), ffn_taps) + ffn_bias, approximate=True
    )
    hidden = (activated * linear.astype(jnp.float32)).astype(jnp.bfloat16)
    full_down = lax.all_gather(w_down, "fs", axis=1, tiled=True)
    partial_two = jnp.dot(hidden, full_down, preferred_element_type=jnp.float32)
    return settle(partial_two, middle_f, ffn_post_gain)


def dot_nt(left, right):
    return lax.dot_general(left, right, (((1,), (1,)), ((), ())), preferred_element_type=jnp.float32)


def dot_nn(left, right):
    return jnp.dot(left, right, preferred_element_type=jnp.float32)


def conv_rows(values, taps):
    height = values.shape[0]
    row = lax.broadcasted_iota(jnp.int32, values.shape, 0) % SEQ_LEN
    before = jnp.where(row == 0, 0.0, pltpu.roll(values, 1, 0))
    after = jnp.where(row == SEQ_LEN - 1, 0.0, pltpu.roll(values, height - 1, 0))
    return taps[0:1] * before + taps[1:2] * values + taps[2:3] * after


def norm_rows(values, gain):
    scale = lax.rsqrt(jnp.mean(values * values, axis=-1, keepdims=True) + EPS)
    return values * scale * gain


def scope(name):
    return jax.named_scope(name) if TRACE else contextlib.nullcontext()


def kernel(n_fs, conv_w, spans, *refs):
    sources, out, scratch = refs[:15], refs[15], refs[16:]
    (
        stream,
        gain_mix_pre,
        gain_mix_post,
        gain_ffn_pre,
        gain_ffn_post,
        mix_taps,
        w_linear,
        w_gated,
        w_down,
        ffn_taps,
        ffn_bias,
        load_s,
        small_all,
        smalls,
        small_pair,
        ffn_w,
        ffn_all,
        mix_all,
        normed,
        acc,
        pm,
        rm,
        sm,
        rxm,
        middle,
        xs,
        pf,
        rf,
        sf,
        rx,
        tf,
        rz,
        rq,
        mz_s,
        mz_r,
        my_s,
        my_r,
        mr_s,
        mr_r,
        fz_s,
        fz_r,
        fy_s,
        fy_r,
        fx_s,
        fx_r,
        az_s,
        az_r,
        ap_s,
        ap_r,
        ac_r,
        rs_s,
        rs_r,
        rp_r,
        rz_r,
        rq_r,
        fin_s,
        fin_r,
    ) = scratch
    r, f, t = lax.axis_index("rep"), lax.axis_index("fs"), lax.axis_index("tp")
    x, c = t // 2, t % 2
    t_core, t_side = 2 * x + 1 - c, 2 * (1 - x) + c
    core, side, other = {"tp": t_core}, {"tp": t_side}, {"rep": 1 - r}
    rows, width = stream.shape[0], ffn_w.shape[3]
    cap, few = ffn_w.shape[2], spans[0][1]
    sizes = (few, cap)
    share = rows // 4
    mine = pl.ds(pl.multiple_of(c * share, share), share)
    theirs = pl.ds(pl.multiple_of((1 - c) * share, share), share)

    near = f < n_fs // 2
    mirror = lambda v: jnp.where(near, v, n_fs - 1 - v)
    inner = jnp.where(near, f, n_fs - 1 - f) == 1
    edge = jnp.logical_not(inner)
    order = [mirror(jnp.where(inner, 0, 1)), mirror(2), mirror(3)]
    goals = [mirror(jnp.where(inner, 2, 1)), mirror(jnp.where(inner, 3, 2)), mirror(jnp.where(inner, 0, 3))]
    upward, downward = mirror(jnp.where(inner, 2, 1)), mirror(0)
    places = [f] + order

    def send(src, dst, ss, rs, where):
        return pltpu.make_async_remote_copy(
            src_ref=src,
            dst_ref=dst,
            send_sem=ss,
            recv_sem=rs,
            device_id=where,
            device_id_type=pl.DeviceIdType.MESH,
        )

    owed = []

    def owe(ref, sem, when=None):
        owed.append((send(ref, ref, sem, sem, core), when))

    def settle_sends():
        for copy, when in owed:
            if when is None:
                copy.wait_send()
            else:
                pl.when(when)(copy.wait_send)

    def begin(copy, when=None):
        if when is None:
            copy.start()
        else:
            pl.when(when)(copy.start)

    def landed(ref, sem, name):
        wait(send(ref, ref, sem, sem, core), name)

    def wait(copy, name):
        with scope(name):
            copy.wait_recv()

    barrier = pltpu.get_barrier_semaphore()
    peers = [core, side, other] + [{"fs": (f + k) % n_fs} for k in (1, 2, 3)]
    for peer in peers:
        pl.semaphore_signal(barrier, inc=1, device_id=peer, device_id_type=pl.DeviceIdType.MESH)
    targets = [mix_all.at[f, p * conv_w : (p + 1) * conv_w] for p in range(4)]
    targets += [stream, gain_mix_pre, w_linear, w_gated, w_down, ffn_taps, ffn_bias]
    targets += [gain_mix_post, gain_ffn_pre, gain_ffn_post, mix_taps]
    places_in = (5, 6, 7, 8, 0, 1, 10, 11, 12, 13, 14, 2, 3, 4, 9)
    loads = [
        pltpu.make_async_copy(sources[i], ref, load_s.at[max(k - 3, 0)])
        for k, (i, ref) in enumerate(zip(places_in, targets))
    ]
    for load in loads:
        load.start()
    pltpu.make_async_copy(mix_all.at[f], mix_all.at[f], load_s.at[0]).wait()
    with scope("barrier"):
        pl.semaphore_wait(barrier, len(peers))

    mix_half = mix_all.shape[1] // 2
    mix_cut = mix_half // CHUNKS

    def mix_copy(b, h, to):
        at = pl.ds(pl.multiple_of(r * mix_half + h * mix_cut, PACK), mix_cut)
        ref = mix_all.at[b, at]
        return send(ref, ref, mz_s.at[0], mz_r.at[b, h], {"fs": to})

    for h in range(CHUNKS):
        begin(mix_copy(f, h, upward))
        begin(mix_copy(f, h, downward), inner)
    owe(mix_all.at[0, 0:mix_half], mz_s.at[0], edge)
    owe(mix_all.at[0:n_fs, 0 : mix_half * 5 // n_fs], mz_s.at[0], inner)

    for load in loads[6:]:
        load.wait()

    pieces = (w_linear, w_gated, w_down)

    def keep(ref, at, size, piece):
        ref[0:size] = piece[at : at + size]
        if size < cap:
            ref[size:cap] = jnp.zeros((cap - size, width), ffn_w.dtype)

    for half in range(2):

        @pl.when(r == half)
        def _():
            for j, (at, *both) in enumerate(spans):
                for p, piece in enumerate(pieces):
                    keep(ffn_w.at[j, p], at + half * both[0], both[half], piece)

    narrow = ((cap, cap, few), (cap, few, few))

    def ffn_send(kind, i):
        for p in range(3):
            at = slice(0, narrow[kind][i])
            src, dst = ffn_w.at[goals[i], p, at], ffn_all.at[f, 0, p, at]
            yield send(src, dst, fz_s.at[i], fz_r.at[f, p], {"fs": goals[i]})

    kinds = (edge, inner)
    ffn_out = [[list(ffn_send(kind, i)) for i in range(3)] for kind in range(2)]
    for kind in range(2):
        for i in range(3):
            owe(ffn_w.at[0, :, 0 : narrow[kind][i]], fz_s.at[i], kinds[kind])

    def ffn_start(kind, *which):
        for i in which:
            for copy in ffn_out[kind][i]:
                copy.start()

    pl.when(edge)(functools.partial(ffn_start, 0, 0, 1, 2))

    own_side = send(ffn_w.at[f], ffn_all.at[f, 2], fx_s.at[0], fx_r.at[0], side)
    own_side.start()
    owe(ffn_w.at[f], fx_s.at[0])
    for p in range(3):
        ffn_all[f, 0, p] = ffn_w[f, p]
    for j, (at, *both) in enumerate(spans):
        for half in range(2):

            @pl.when((f == j) & (r == half))
            def _():
                for p, piece in enumerate(pieces):
                    keep(ffn_all.at[j, 1, p], at + (1 - half) * both[0], both[1 - half], piece)

    @pl.when(edge)
    def _():
        for i in range(1, 4):
            ffn_all[places[i], :, :, few:cap] = jnp.zeros((3, 3, cap - few, width), ffn_w.dtype)

    small_all[...] = jnp.zeros(small_all.shape, jnp.float32)
    for j, (first, *both) in enumerate(spans):
        for half, size in enumerate(both):
            at = first + half * both[0]
            small_all[j, half, 0:3, 0:size] = ffn_taps[:, at : at + size]
            small_all[j, half, 3:4, 0:size] = ffn_bias[at : at + size][None]
    smalls[0] = small_all[f, r]
    smalls[1] = small_all[f, 1 - r]
    small_copy = send(smalls.at[0], smalls.at[2], fx_s.at[1], fx_r.at[1], side)
    small_copy.start()
    owe(smalls.at[0], fx_s.at[1])

    for load in loads[4:6]:
        load.wait()
    step_rows = 32

    @pl.loop(0, rows // step_rows)
    def _(i):
        at = pl.ds(pl.multiple_of(i * step_rows, step_rows), step_rows)
        value = norm_rows(stream[at].astype(jnp.float32), gain_mix_pre[...][None]).astype(jnp.bfloat16)
        for j in range(n_fs):
            normed[j, at] = value[:, j * width : (j + 1) * width]

    def project(z, first=False):
        for p in range(3):
            term = dot_nt(normed[z], mix_all[z, p * conv_w : (p + 1) * conv_w])
            acc[p] = term if first else acc[p] + term

    project(f, True)

    flows = [(i, h) for i in range(3) for h in range(CHUNKS)]
    turns = [(i, h) for h in range(CHUNKS) for i in range(2)] + [(2, h) for h in range(CHUNKS)]
    my = []
    for e in range(3 * CHUNKS):
        (i_edge, h_edge), (i_inner, h_inner) = flows[e], turns[e]
        b = jnp.where(inner, order[i_inner], order[i_edge])
        h = jnp.where(inner, h_inner, h_edge)
        onward = downward if i_inner > 0 else upward
        copy = mix_copy(b, h, onward)
        wait(copy, f"mixz_{e}")
        begin(copy, inner)
        at = pl.ds(pl.multiple_of(r * mix_half + h * mix_cut, PACK), mix_cut)
        ref = mix_all.at[b, at]
        my.append(send(ref, ref, my_s.at[0], my_r.at[e], other))
        my[e].start()
        if e == 2 * CHUNKS - 2:
            pl.when(inner)(functools.partial(ffn_start, 1, *FIRST))
    owe(mix_all.at[0:3, 0:mix_half], my_s.at[0])
    pl.when(inner)(functools.partial(ffn_start, 1, 2))

    def hop(kind, i, p, piece, ss, rs, to):
        src = ffn_all.at[places[i], 0, p, 0 : sizes[kind]]
        dst = ffn_all.at[places[i], piece, p, 0 : sizes[kind]]
        return send(src, dst, ss, rs, to)

    trips = [(i, p) for i in range(1, 4) for p in range(3)]
    fy = [{(i, p): hop(kind, i, p, 1, fy_s.at[0], fy_r.at[0], other) for i, p in trips} for kind in range(2)]
    fx = [{(i, p): hop(kind, i, p, 2, fx_s.at[2], fx_r.at[2], side) for i, p in trips} for kind in range(2)]
    all_trips = [ffn_all.at[0:3, 0, :, 0 : sizes[kind]] for kind in range(2)]
    for kind in range(2):
        owe(all_trips[kind], fy_s.at[0], kinds[kind])
        owe(all_trips[kind], fx_s.at[2], kinds[kind])

    def forward(kind, *which):
        for i, p in which:
            src = ffn_all.at[places[i], 0, p, 0 : sizes[kind]]
            wait(send(src, src, fz_s.at[i - 1], fz_r.at[places[i], p], other), f"ffnz_{i}_{p}")
            fy[kind][i, p].start()
            fx[kind][i, p].start()

    def relay(edge_list, inner_list):
        for kind, which in enumerate((edge_list, inner_list)):
            if which:
                pl.when(kinds[kind])(functools.partial(forward, kind, *which))

    def arrived(kind):
        landed(all_trips[kind], fy_r.at[0], "ffny")
        landed(all_trips[kind], fx_r.at[2], "ffnx")

    relay(EDGE[0], INNER[0])
    for e in range(3 * CHUNKS):
        if e == 2 * CHUNKS:
            relay(EDGE[1], INNER[1])
        wait(my[e], f"mixy_{e}")
        if e == 2 * CHUNKS - 1:
            project(order[0])
            project(order[1])
    project(order[2])

    mix_core = []
    for k, q in enumerate((1 - x, x)):
        here = pl.ds(pl.multiple_of(q * SEQ_LEN, SEQ_LEN), SEQ_LEN)
        parts = [acc[p, here].astype(jnp.bfloat16).astype(jnp.float32) for p in range(3)]
        mixed = (parts[0] * conv_rows(parts[1] * parts[2], mix_taps)).astype(jnp.bfloat16)
        for j in range(n_fs):
            pm[k, :, j * width : (j + 1) * width] = dot_nn(
                mixed, mix_all[j, 3 * conv_w : 4 * conv_w]
            ).astype(jnp.bfloat16)
        mix_core.append(send(pm.at[k, theirs], rm.at[k], mr_s.at[0], mr_r.at[k], core))
        mix_core[k].start()

    def mix_sum(k):
        wait(mix_core[k], f"mixcore_{k}")
        return (pm[k, mine].astype(jnp.float32) + rm[k].astype(jnp.float32)).astype(jnp.bfloat16)

    sm[...] = mix_sum(0)
    mix_side = send(sm, rxm, mr_s.at[0], mr_r.at[2], side)
    mix_side.start()
    owe(rz.at[0:3], mr_s.at[0])

    kept = mix_sum(1)
    relay(EDGE[2], INNER[2])
    wait(mix_side, "mixside")
    branch = (kept.astype(jnp.float32) + rxm[...].astype(jnp.float32)).astype(jnp.bfloat16)
    slot = pl.ds(pl.multiple_of(t * share, share), share)
    mid = stream[slot].astype(jnp.float32) + norm_rows(branch.astype(jnp.float32), gain_mix_post[...][None])
    mid = mid.astype(jnp.bfloat16)
    middle[...] = mid
    xs[f, 0, mine] = norm_rows(mid.astype(jnp.float32), gain_ffn_pre[...][None]).astype(jnp.bfloat16)

    sideways = [jnp.where(edge, a, b) for a, b in zip(*SIDEWAYS)]
    partner = [{"rep": jnp.where(a, r, 1 - r), "tp": jnp.where(a, t_side, t)} for a in sideways]
    cut = share // SPREAD

    def piece_of(z, s, a):
        return xs.at[z, s, pl.ds(pl.multiple_of(c * share + a * cut, cut), cut)]

    ag_core, ag_pair, ag_pass = {}, {}, {}

    slab = pl.ds(pl.multiple_of(c * share, share), share)
    slab_core = pl.ds(pl.multiple_of((1 - c) * share, share), share)
    for i in range(4):
        for a in range(SPREAD):
            src, far = piece_of(places[i], 0, a), piece_of(places[i], 1, a)
            ag_pair[i, a] = send(src, far, ap_s.at[0], ap_r.at[i, a], partner[i])
            ag_core[i, a] = send(src, src, ap_s.at[1], ac_r.at[0, i], core)
            ag_pass[i, a] = send(far, far, ap_s.at[2], ac_r.at[1, i], core)
    for k in range(3):
        owe(rz, ap_s.at[k])
    owe(rz.at[0], az_s.at[0])
    owe(rz, az_s.at[1], inner)

    def pair_own():
        for a in range(SPREAD):
            ag_pair[0, a].start()

    def spread(i, which=range(SPREAD)):
        for a in which:
            src = piece_of(places[i], 0, a)
            if i == 0:
                send(src, src, az_s.at[0], az_r.at[f, a], {"fs": upward}).start()
                begin(send(src, src, az_s.at[1], az_r.at[f, a], {"fs": downward}), inner)
            else:
                copy = send(src, src, az_s.at[1], az_r.at[places[i], a], {"fs": downward if i > 1 else upward})
                wait(copy, f"agz_{i}_{a}")
                begin(copy, inner)
                ag_pair[i, a].start()
            ag_core[i, a].start()

    def pass_on(i):
        for a in range(SPREAD):
            wait(ag_pair[i, a], f"agpair_{i}_{a}")
            ag_pass[i, a].start()

    rs_core, rs_pair = {}, {}
    part = share // PARTS

    def activate(linear, gated, small):
        linear = linear.astype(jnp.bfloat16).astype(jnp.float32)
        gated = gated.astype(jnp.bfloat16).astype(jnp.float32)
        act = jax.nn.gelu(conv_rows(gated, small) + small[3:4], approximate=True)
        return (act * linear).astype(jnp.bfloat16)

    def raise_up(z, weights):
        linear, gated = 0.0, 0.0
        for j in range(0, n_fs, JOIN):
            act = xs[z, :, :, j * width : (j + JOIN) * width].reshape(2 * SEQ_LEN, JOIN * width)
            joined = lambda p: jnp.concatenate([weights(j + k, p) for k in range(JOIN)], axis=1)
            linear = linear + dot_nt(act, joined(0))
            gated = gated + dot_nt(act, joined(1))
        return linear, gated

    def keep_partial(i, j, total):
        pf[i, :, :, j * width : (j + 1) * width] = total.astype(jnp.bfloat16).reshape(2, SEQ_LEN, width)

    def block_edge(i):
        second = 1 if SIDEWAYS[0][i] else 2
        both = lambda j, p: jnp.concatenate([ffn_all[j, h, p, 0:few] for h in (0, second)], axis=0)
        hidden = activate(*raise_up(places[i], both), small_pair[second - 1])
        for j in range(n_fs):
            keep_partial(i, j, dot_nn(hidden, both(j, 2)))

    def block_inner(i):
        second = 1 if SIDEWAYS[1][i] else 2
        hidden = [
            activate(*raise_up(places[i], lambda j, p: ffn_all[j, h, p]), smalls[h]) for h in (0, second)
        ]
        for j in range(n_fs):
            total = dot_nn(hidden[0], ffn_all[j, 0, 2]) + dot_nn(hidden[1], ffn_all[j, second, 2])
            keep_partial(i, j, total)

    def block(i):
        for s in range(2):
            landed(xs.at[places[i], s, slab_core], ac_r.at[s, i], f"agcore_{i}_{s}")
        for kind in range(2):
            pl.when(kinds[kind])(functools.partial((block_edge, block_inner)[kind], i))
        for s in (1, 0):
            rs_core[i, s] = send(pf.at[i, s, theirs], rf.at[i, s], rs_s.at[0], rs_r.at[i, s], core)
            rs_core[i, s].start()

    def stage_core(i, s):
        wait(rs_core[i, s], f"rscore_{i}_{s}")
        for a in range(PARTS):
            at = pl.ds(a * part, part)
            ours = pl.ds(pl.multiple_of(c * share + a * part, part), part)
            total = pf[i, s, ours].astype(jnp.float32) + rf[i, s, at].astype(jnp.float32)
            sf[i, s, at] = total.astype(jnp.bfloat16)
            if s:
                rs_pair[i, a] = send(sf.at[i, s, at], rx.at[i, at], rs_s.at[1], rp_r.at[i, a], partner[i])
                rs_pair[i, a].start()

    rs_line = {}
    for i in range(1, 4):
        for a in range(PARTS):
            at = pl.ds(a * part, part)
            home = send(tf.at[i, at], rz.at[f, at], rs_s.at[2], rz_r.at[f, a], {"fs": places[i]})
            near_by = None
            if i > 1:
                near_by = send(tf.at[i, at], rq.at[i, at], rs_s.at[2], rq_r.at[i - 2, a], {"fs": places[1]})
            rs_line[i, a] = home, near_by
    owe(xs.at[:, 0], rs_s.at[0])
    owe(rz, rs_s.at[1])
    owe(rz.at[0:3], rs_s.at[2])

    def stage_pair(i, which=range(PARTS)):
        for a in which:
            at = pl.ds(a * part, part)
            wait(rs_pair[i, a], f"rspair_{i}_{a}")
            total = sf[i, 0, at].astype(jnp.float32) + rx[i, at].astype(jnp.float32)
            if i == 0:
                tf[i, at] = total.astype(jnp.bfloat16)
                continue
            home, near_by = rs_line[i, a]
            if near_by is None:
                tf[i, at] = total.astype(jnp.bfloat16)
                home.start()
                continue

            @pl.when(edge)
            def _():
                tf[i, at] = total.astype(jnp.bfloat16)
                near_by.start()

            @pl.when(inner)
            def _():
                wait(near_by, f"rq_{i}_{a}")
                tf[i, at] = (total + rq[i, at].astype(jnp.float32)).astype(jnp.bfloat16)
                home.start()

    def stage(i):
        stage_core(i, 1)
        stage_core(i, 0)

    spread(0)
    relay(EDGE[3], INNER[3])

    @pl.when(edge)
    def _():
        spread(1)
        pair_own()
        spread(2)
        pass_on(1)
        arrived(0)

    @pl.when(inner)
    def _():
        spread(1)
        spread(2)
        spread(3)
        pair_own()
        pass_on(1)
        arrived(1)

    wait(own_side, "ffnown")
    wait(small_copy, "small")
    for k in range(2):
        small_pair[k, :, 0:few] = smalls[0, :, 0:few]
        small_pair[k, :, few : 2 * few] = smalls[k + 1, :, 0:few]
    block(1)
    pl.when(edge)(functools.partial(spread, 3))
    pass_on(2)
    stage(1)
    block(2)
    pass_on(3)
    stage_pair(1, (0,))
    stage(2)
    stage_pair(1, (1,))
    block(3)
    stage_pair(1, range(2, PARTS))
    pass_on(0)
    stage(3)
    pl.when(edge)(functools.partial(stage_pair, 2, (0,)))
    block(0)
    pl.when(edge)(functools.partial(stage_pair, 2, range(1, PARTS)))
    stage(0)
    pl.when(inner)(functools.partial(stage_pair, 2))
    stage_pair(3)
    stage_pair(0)

    def row_slot(who, a):
        return pl.ds(pl.multiple_of(who * share + a * part, part), part)

    fin = {}
    for a in range(PARTS):
        at = pl.ds(a * part, part)
        total = tf[0, at].astype(jnp.float32)
        for i in range(1, 3):
            ref = rz.at[places[i], at]
            landed(ref, rz_r.at[places[i], a], f"rz_{i}_{a}")
            total = total + rz[places[i], at].astype(jnp.float32)
        branch = total.astype(jnp.bfloat16).astype(jnp.float32)
        done = middle[at].astype(jnp.float32) + norm_rows(branch, gain_ffn_post[...][None])
        out[row_slot(t, a)] = done.astype(jnp.bfloat16)
        own = out.at[row_slot(t, a)]
        fin[a] = send(own, own, fin_s.at[0], fin_r.at[a], side)
        fin[a].start()
        send(own, own, fin_s.at[0], fin_r.at[PARTS], core).start()
    for a in range(PARTS):
        wait(fin[a], f"finside_{a}")
        far = out.at[row_slot(t_side, a)]
        send(far, far, fin_s.at[0], fin_r.at[PARTS + 1], core).start()
    for k in range(2):
        landed(rz.at[0], fin_r.at[PARTS + k], f"fincore_{k}")
    owe(rz.at[0:3], fin_s.at[0])
    settle_sends()


def split_plan(
    n_fs,
    stream,
    mix_pre_gain,
    w_outer_gate,
    w_inner_gate,
    w_value,
    mix_taps,
    w_mix_out,
    mix_post_gain,
    ffn_pre_gain,
    w_linear,
    w_gated,
    ffn_taps,
    ffn_bias,
    w_down,
    ffn_post_gain,
):
    rows, model = stream.shape
    width, conv_w = w_value.shape
    tiles = w_linear.shape[1] // (2 * PACK)
    few = tiles * 7 // 32 * PACK
    more = tiles * PACK - 2 * few
    cap = -(-more // (2 * PACK)) * PACK
    spans, at = [], 0
    for z in range(n_fs):
        both = (few, few) if z in (0, n_fs - 1) else (cap, more - cap)
        spans.append((at, *both))
        at += sum(both)
    share = rows // 4
    half = jnp.bfloat16
    vmem, dma = pltpu.VMEM, pltpu.SemaphoreType.DMA
    return pl.pallas_call(
        functools.partial(kernel, n_fs, conv_w, tuple(spans)),
        out_shape=pltpu.VMEM((rows, model), half),
        in_specs=[pl.BlockSpec(memory_space=pltpu.HBM)] * 15,
        out_specs=pl.BlockSpec(memory_space=vmem),
        scratch_shapes=[
            vmem((rows, model), half),
            vmem((model,), jnp.float32),
            vmem((model,), jnp.float32),
            vmem((model,), jnp.float32),
            vmem((model,), jnp.float32),
            vmem(mix_taps.shape, jnp.float32),
            vmem(w_down.shape, half),
            vmem(w_down.shape, half),
            vmem(w_down.shape, half),
            vmem(ffn_taps.shape, jnp.float32),
            vmem(ffn_bias.shape, jnp.float32),
            dma((12,)),
            vmem((n_fs, 2, 8, cap), jnp.float32),
            vmem((3, 8, cap), jnp.float32),
            vmem((2, 8, 2 * few), jnp.float32),
            vmem((n_fs, 3, cap, width), half),
            vmem((n_fs, 3, 3, cap, width), half),
            vmem((n_fs, 4 * conv_w, width), half),
            vmem((n_fs, rows, width), half),
            vmem((3, rows, conv_w), jnp.float32),
            vmem((2, SEQ_LEN, model), half),
            vmem((2, share, model), half),
            vmem((share, model), half),
            vmem((share, model), half),
            vmem((share, model), half),
            vmem((n_fs, 2, SEQ_LEN, model), half),
            vmem((n_fs, 2, SEQ_LEN, model), half),
            vmem((n_fs, 2, share, model), half),
            vmem((n_fs, 2, share, model), half),
            vmem((n_fs, share, model), half),
            vmem((n_fs, share, model), half),
            vmem((n_fs, share, model), half),
            vmem((n_fs, share, model), half),
            dma((1,)),
            dma((n_fs, CHUNKS)),
            dma((1,)),
            dma((3 * CHUNKS,)),
            dma((1,)),
            dma((3,)),
            dma((3,)),
            dma((n_fs, 3)),
            dma((1,)),
            dma((1,)),
            dma((3,)),
            dma((3,)),
            dma((2,)),
            dma((n_fs, SPREAD)),
            dma((3,)),
            dma((n_fs, SPREAD)),
            dma((2, n_fs)),
            dma((3,)),
            dma((n_fs, 2)),
            dma((n_fs, PARTS)),
            dma((n_fs, PARTS)),
            dma((2, PARTS)),
            dma((1,)),
            dma((PARTS + 2,)),
        ],
        compiler_params=pltpu.CompilerParams(
            collective_id=0, has_side_effects=True, vmem_limit_bytes=58 * 2**20
        ),
    )(
        stream,
        mix_pre_gain,
        mix_post_gain,
        ffn_pre_gain,
        ffn_post_gain,
        w_outer_gate.T,
        w_inner_gate.T,
        w_value.T,
        w_mix_out,
        mix_taps,
        w_linear.T,
        w_gated.T,
        w_down,
        ffn_taps,
        ffn_bias,
    )


def on_device(rep, n_fs, n_tp, *arrays):
    stream, w_value, w_linear = arrays[0], arrays[4], arrays[9]
    same = n_fs == n_tp == 2 * rep == 4
    whole = w_value.shape[0] % 128 == 0 and 2 * w_value.shape[1] % (CHUNKS * PACK) == 0
    even = w_linear.shape[1] % (2 * PACK) == 0 and stream.shape[0] == 2 * SEQ_LEN
    if same and whole and even:
        return split_plan(n_fs, *arrays)
    return gather_plan(*arrays)


def solution(mesh):
    in_specs = (
        P(("rep", "fs"), None),
        P(),
        P("fs", "tp"),
        P("fs", "tp"),
        P("fs", "tp"),
        P(None, "tp"),
        P("tp", "fs"),
        P(),
        P(),
        P("fs", "tp"),
        P("fs", "tp"),
        P(None, "tp"),
        P("tp"),
        P("tp", "fs"),
        P(),
    )
    out_specs = P(("rep", "fs"), None)
    sizes = mesh.shape
    body = functools.partial(on_device, sizes["rep"], sizes["fs"], sizes["tp"])
    return jax.shard_map(
        body, mesh=mesh, in_specs=in_specs, out_specs=out_specs, check_vma=False
    )
```
